32 devices in a mesh: sp: 8 (over z, x), tp: 4 (over y, core).
Axes of the slice: x: 2, y: 2, z: 4, core: 2. Of those that a mesh axis runs over, the one named last changes fastest.
Arguments:
- residual_matrix: bfloat16 [2048, 2048], P(('sp', 'tp')), may hold values from -6 to 6
- query_vectors: bfloat16 [2048, 2048], P('tp', 'sp'), may hold values from -6 to 6
- lookup_vectors: bfloat16 [2048, 2048], P('tp', 'sp'), may hold values from -6 to 6
- payload_vectors: bfloat16 [2048, 2048], P('tp', 'sp'), may hold values from -6 to 6
- fading_dependent_term: bfloat16 [2048, 2048], P('tp', 'sp'), may hold values from -4 to 4
- step_size_preactivation: bfloat16 [2048, 2048], P('tp', 'sp'), may hold values from -8 to 8
- attention_result_switch: bfloat16 [2048, 2048], P('tp', 'sp'), may hold values from -6 to 6
- fading_bias_vector: float32 [2048], P('tp'), may hold values from -16 to -2
- surplus_forgetting: float32 [32, 2048], P('tp', 'sp'), may hold values from -0.7 to 0
- per_group_scaler: float32 [2048], P('tp'), may hold values from 0.1 to 1.9
- attention_result_matrix: bfloat16 [2048, 2048], P('tp'), may hold values from -0.125 to 0.125
- dense_block_scaler: float32 [2048], replicated, may hold values from 0.1 to 1.9
- switching_matrix: bfloat16 [2048, 5632], P('sp', 'tp'), may hold values from -0.125 to 0.125
- expanding_matrix: bfloat16 [2048, 5632], P('sp', 'tp'), may hold values from -0.125 to 0.125
- contracting_matrix: bfloat16 [5632, 2048], P('tp', 'sp'), may hold values from -0.078125 to 0.078125
Outputs:
- blended: bfloat16 [2048, 2048], P(('sp', 'tp'))
The draws below stay inside these ranges and needn't reach their ends.
All inputs are finite; a program needn't handle non-finite values.
Results may differ from the reference program's by a relative error of at most 0.015.
Values may be sent and summed in bfloat16 or wider, within the bound.
A program may use at most 128 MiB of HBM per device.

```python
import math
import jax
import jax.numpy as jnp
from jax import lax

D = 2048
HEAD = 64
HEADS = 32
FF = 5632
BLOCK = 64
TOK_DEV = 256
MIX = 2048
TOKENS = 2048
N_TP = 4


def draw_lookup_vectors(key, part):
    noise_key = jax.random.fold_in(key, 41)
    quiet_key = jax.random.fold_in(key, 42)
    level_key = jax.random.fold_in(key, 43)
    direction_key = jax.random.fold_in(key, 44)
    block_key = jax.random.fold_in(key, 45)
    noise = jnp.clip(jax.random.normal(noise_key, (HEADS, HEAD, TOKENS), jnp.float32), -5.0, 5.0)
    quiet = jax.random.uniform(quiet_key, (HEADS, HEAD, 1), jnp.float32) < 0.25
    quiet_level = jnp.exp(jax.random.uniform(level_key, (HEADS, HEAD, 1), jnp.float32, math.log(0.01), math.log(0.05)))
    position = jnp.arange(TOKENS)[None, None, :]
    later = position >= TOK_DEV
    factor = jnp.where(jnp.logical_and(quiet, later), quiet_level, 1.0)
    direction = jax.random.normal(direction_key, (HEADS, HEAD, 1), jnp.float32)
    direction = direction * (3.0 / jnp.sqrt(jnp.sum(direction * direction, axis=1, keepdims=True) + 1e-06))
    chosen = jax.random.uniform(block_key, (HEADS, 1, TOKENS // BLOCK), jnp.float32) < 0.25
    chosen = jnp.repeat(chosen, BLOCK, axis=2)
    keys = (noise + jnp.where(chosen, direction, 0.0)) * factor
    return jnp.clip(keys, -6.0, 6.0).reshape(MIX, TOKENS).astype(jnp.bfloat16)


def draw_fading_bias_vector(key, part):
    first_key = jax.random.fold_in(key, 11)
    second_key = jax.random.fold_in(key, 12)
    fast_share = 0.5
    fast_heads = jax.random.uniform(first_key, (HEADS, 1), jnp.float32) < fast_share
    jitter = jax.random.uniform(second_key, (HEADS, HEAD), jnp.float32, -0.5, 0.5)
    slow_level = math.log(0.6 / TOKENS) + 0.5
    return (jnp.where(fast_heads, -3.4, slow_level) + jitter).reshape(HEADS * HEAD).astype(jnp.float32)


def draw_fading_dependent_term(key, part):
    first_key = jax.random.fold_in(key, 21)
    second_key = jax.random.fold_in(key, 22)
    noise = jnp.clip(jax.random.normal(first_key, (MIX, TOKENS), jnp.float32) * 0.7, -3.0, 3.0)
    levels = jax.random.uniform(second_key, (TOKENS // TOK_DEV,), jnp.float32, -0.7, 0.7)
    return (noise + jnp.repeat(levels, TOK_DEV)[None, :]).astype(jnp.bfloat16)


def draw_surplus_forgetting(key, part):
    first_key = jax.random.fold_in(key, 31)
    second_key = jax.random.fold_in(key, 32)
    struck = jax.random.uniform(first_key, (HEADS, TOKENS), jnp.float32) < 3.0 / TOKENS
    losses = jnp.log(jax.random.uniform(second_key, (HEADS, TOKENS), jnp.float32, 0.5, 0.8))
    return jnp.where(struck, losses, 0.0).astype(jnp.float32)


def shard_levels(own_key, extent, shards, smallest, high):
    factor_of = 1.0
    for dim, shards_of in shards:
        heights = jax.random.uniform(jax.random.fold_in(jax.random.fold_in(own_key, 6), dim), (shards_of,), jnp.float32, smallest / len(shards), high / len(shards))
        factor_of = factor_of * jnp.repeat(jnp.exp(heights), extent[dim] // shards_of).reshape((-1,) + (1,) * (len(extent) - 1 - dim))
    return factor_of


def bell_draw(key, extent, spread, limit, split=(), kind=jnp.bfloat16):
    entries = spread * jax.random.normal(key, extent, jnp.float32)
    if split:
        entries = entries * shard_levels(key, extent, split, -0.22, 0.18)
    return jnp.clip(entries, -limit, limit).astype(kind)


def setup_inputs(seed: int = 0) -> dict:
    streams_of = jax.random.split(jax.random.key(seed), 16)
    residual_matrix = bell_draw(streams_of[0], (TOKENS, D), 1.0, 6.0, ((0, 32),))
    query_vectors = bell_draw(streams_of[1], (MIX, TOKENS), 1.0, 6.0, ((0, 4), (1, 8)))
    lookup_vectors = draw_lookup_vectors(jax.random.fold_in(streams_of[15], 71), 0)
    payload_vectors = bell_draw(streams_of[3], (MIX, TOKENS), 1.0, 6.0, ((0, 4), (1, 8)))
    fading_dependent_term = draw_fading_dependent_term(jax.random.fold_in(streams_of[15], 71), 0)
    step_size_preactivation = bell_draw(streams_of[5], (MIX, TOKENS), 1.5, 8.0, ((0, 4), (1, 8)))
    attention_result_switch = bell_draw(streams_of[6], (MIX, TOKENS), 1.0, 6.0, ((0, 4), (1, 8)))
    fading_bias_vector = draw_fading_bias_vector(jax.random.fold_in(streams_of[15], 71), 0)
    surplus_forgetting = draw_surplus_forgetting(jax.random.fold_in(streams_of[15], 71), 0)
    per_group_scaler = jnp.clip(1.0 + 0.18 * jax.random.normal(streams_of[9], (MIX,), jnp.float32), 0.1, 1.9)
    attention_result_matrix = bell_draw(streams_of[10], (MIX, D), MIX ** -0.5, 0.125, ((0, 4),))
    dense_block_scaler = jnp.clip(1.0 + 0.18 * jax.random.normal(streams_of[11], (D,), jnp.float32), 0.1, 1.9)
    switching_matrix = bell_draw(streams_of[12], (D, FF), D ** -0.5, 0.125, ((0, 8), (1, 4)))
    expanding_matrix = bell_draw(streams_of[13], (D, FF), D ** -0.5, 0.125, ((0, 8), (1, 4)))
    contracting_matrix = bell_draw(streams_of[14], (FF, D), FF ** -0.5, 0.078125, ((0, 4), (1, 8)))
    return dict(residual_matrix=residual_matrix, query_vectors=query_vectors, lookup_vectors=lookup_vectors, payload_vectors=payload_vectors, fading_dependent_term=fading_dependent_term, step_size_preactivation=step_size_preactivation, attention_result_switch=attention_result_switch, fading_bias_vector=fading_bias_vector, surplus_forgetting=surplus_forgetting, per_group_scaler=per_group_scaler, attention_result_matrix=attention_result_matrix, dense_block_scaler=dense_block_scaler, switching_matrix=switching_matrix, expanding_matrix=expanding_matrix, contracting_matrix=contracting_matrix)


norm_eps = 1e-06
group_eps = 0.00064
key_eps = 1e-06
highest = lax.Precision.HIGHEST

def per_token(source):
    return source.astype(jnp.float32).reshape(HEADS, HEAD, TOKENS).transpose(2, 0, 1)

def reference(residual_matrix, query_vectors, lookup_vectors, payload_vectors, fading_dependent_term, step_size_preactivation, attention_result_switch, fading_bias_vector, surplus_forgetting, per_group_scaler, attention_result_matrix, dense_block_scaler, switching_matrix, expanding_matrix, contracting_matrix):
    read_rows = per_token(query_vectors)
    key_rows = per_token(lookup_vectors)
    value_rows = per_token(payload_vectors)
    fading_preactivation = per_token(fading_dependent_term) + fading_bias_vector.reshape(HEADS, HEAD)[None]
    log_fading_factor = -jnp.exp(-jax.nn.softplus(-fading_preactivation) - 0.5) + surplus_forgetting.T[:, :, None]
    learn_rate = jax.nn.sigmoid(per_token(step_size_preactivation))
    unit_keys = key_rows * lax.rsqrt(lax.optimization_barrier(jnp.sum(key_rows * key_rows, axis=-1, keepdims=True)) + key_eps)
    scaled = key_rows * learn_rate
    removal = unit_keys * learn_rate

    def advance(carried, member):
        read_step, decay_step, unit_step, removal_step, key_step, value_step = member
        seen_part = jnp.einsum('hij,hj->hi', carried, unit_step, precision=highest)
        carried = carried * decay_step[:, None, :] - seen_part[:, :, None] * removal_step[:, None, :] + value_step[:, :, None] * key_step[:, None, :]
        return (carried, jnp.einsum('hij,hj->hi', carried, read_step, precision=highest))
    zero_state = jnp.zeros((HEADS, HEAD, HEAD), jnp.float32)
    _, outputs = lax.scan(advance, zero_state, (read_rows, jnp.exp(log_fading_factor), unit_keys, removal, scaled, value_rows))
    centred = outputs - lax.optimization_barrier(jnp.mean(outputs, axis=-1, keepdims=True))
    variance = lax.optimization_barrier(jnp.mean(centred * centred, axis=-1, keepdims=True))
    normed_heads = (centred * lax.rsqrt(variance + group_eps)).reshape(TOKENS, HEADS * HEAD)
    mixed_out = (normed_heads * per_group_scaler[None, :] * attention_result_switch.astype(jnp.float32).T).astype(jnp.bfloat16)
    middle = residual_matrix.astype(jnp.float32) + jnp.dot(mixed_out, attention_result_matrix, preferred_element_type=jnp.float32)
    normed = (middle * lax.rsqrt(lax.optimization_barrier(jnp.mean(middle * middle, axis=-1, keepdims=True)) + norm_eps) * dense_block_scaler).astype(jnp.bfloat16)
    gate_sum = jnp.dot(normed, switching_matrix, preferred_element_type=jnp.float32)
    up_sum = jnp.dot(normed, expanding_matrix, preferred_element_type=jnp.float32)
    hidden = (jax.nn.silu(gate_sum) * up_sum).astype(jnp.bfloat16)
    group_width = FF // N_TP

    def add_group(total_sum, group_index):
        piece_rows = lax.dynamic_slice_in_dim(hidden, group_index * group_width, group_width, 1)
        down_rows = lax.dynamic_slice_in_dim(contracting_matrix, group_index * group_width, group_width, 0)
        product = jnp.dot(piece_rows, down_rows, preferred_element_type=jnp.float32)
        rounded = lax.optimization_barrier(product.astype(jnp.bfloat16))
        return (total_sum + rounded.astype(jnp.float32), None)
    channel_out, _ = lax.scan(add_group, jnp.zeros((TOKENS, D), jnp.float32), jnp.arange(N_TP, dtype=jnp.int32))
    return (middle + channel_out).astype(jnp.bfloat16)
```

```python
import functools
import jax
import jax.numpy as jnp
from jax import lax
from jax.experimental import pallas as pl
from jax.experimental.pallas import tpu as pltpu
from jax.sharding import PartitionSpec as P

HEAD = 64
BLOCK = 64


norm_eps = 1e-06
group_eps = 0.00064
key_eps = 1e-06
highest = lax.Precision.HIGHEST
high = lax.Precision.HIGH


def shifted(x, axis, by):
    n = lax.axis_size(axis)
    return lax.ppermute(x, axis, [(i, (i + by) % n) for i in range(n)])


def paired(x):
    n = lax.axis_size("sp")
    return lax.ppermute(x, "sp", [(i, i ^ 1) for i in range(n)])


def around(first, second):
    n = lax.axis_size("sp")
    ring = n // 2
    half = ring // 2

    def hop(x, by):
        return lax.ppermute(x, "sp", [(i, (i + 2 * by) % n) for i in range(n)])

    out = [[None] * ring, [None] * ring]
    for place, piece in enumerate((first, second)):
        out[place][0] = piece
        up = down = piece
        for step in range(1, half):
            up = hop(up, 1)
            down = hop(down, -1)
            out[place][ring - step] = up
            out[place][step] = down
        if ring > 1:
            out[place][half] = hop(up, 1) if place == 0 else hop(down, -1)
    return out


def rolled(x, by):
    return lax.dynamic_slice_in_dim(jnp.concatenate([x, x], axis=1), by, x.shape[1], 1)


def carried_in(summary):
    n = lax.axis_size("sp")
    carry_map, carry_add = summary
    both = jnp.concatenate([carry_map, carry_add], axis=1).astype(jnp.bfloat16)
    width = carry_map.shape[1]
    state = jnp.zeros_like(carry_add)
    for back in range(n - 1, 0, -1):
        came = lax.ppermute(both, "sp", [(i, i + back) for i in range(n - back)])
        came = came.astype(jnp.float32)
        state = (
            jnp.einsum("hvk,hkj->hvj", state, came[:, :width], precision=high)
            + came[:, width:]
        )
    return state


def by_blocks(source, attention_group_count, position_count):
    return (
        source.astype(jnp.float32)
        .reshape(attention_group_count, HEAD, position_count // BLOCK, BLOCK)
        .transpose(0, 2, 3, 1)
    )


def compose(earlier, latter):
    return (
        jnp.einsum("...ij,...jk->...ik", earlier[0], latter[0], precision=high),
        jnp.einsum("...ij,...jk->...ik", earlier[1], latter[0], precision=high) + latter[1],
    )


def unit_lower_solve(mutual, right_side):
    power = -mutual
    solved = right_side
    for level in range((BLOCK - 1).bit_length()):
        solved = solved + jnp.einsum("hbts,hbsn->hbtn", power, solved, precision=highest)
        if level + 1 < (BLOCK - 1).bit_length():
            power = jnp.einsum("hbts,hbsu->hbtu", power, power, precision=highest)
    return solved


def rms_rows(middle, dense_block_scaler):
    scale_rows = lax.rsqrt(jnp.mean(middle * middle, axis=-1, keepdims=True) + norm_eps)
    return (middle * scale_rows * dense_block_scaler).astype(jnp.bfloat16)


def local(
    residual_matrix,
    query_vectors,
    lookup_vectors,
    payload_vectors,
    fading_dependent_term,
    step_size_preactivation,
    attention_result_switch,
    fading_bias_vector,
    surplus_forgetting,
    per_group_scaler,
    attention_result_matrix,
    dense_block_scaler,
    switching_matrix,
    expanding_matrix,
    contracting_matrix,
):
    count_sp, count_tp = lax.axis_size("sp"), lax.axis_size("tp")
    parity = lax.axis_index("sp") % 2
    ring_place = lax.axis_index("sp") // 2
    units = switching_matrix.shape[1] // 2

    def part(x, which, axis):
        return lax.dynamic_slice_in_dim(x, which * units, units, axis)

    def gate_up(which):
        return jnp.concatenate(
            [part(switching_matrix, which, 1), part(expanding_matrix, which, 1)], axis=1
        )

    wide_pieces = around(gate_up(parity), paired(gate_up(1 - parity)))
    down_pieces = around(
        part(contracting_matrix, parity, 0), part(contracting_matrix, 1 - parity, 0)
    )
    attention_group_count = surplus_forgetting.shape[0]
    position_count = surplus_forgetting.shape[1]
    block_count = position_count // BLOCK
    read_rows = by_blocks(query_vectors, attention_group_count, position_count)
    key_rows = by_blocks(lookup_vectors, attention_group_count, position_count)
    value_rows = by_blocks(payload_vectors, attention_group_count, position_count)
    fading_preactivation = by_blocks(
        fading_dependent_term, attention_group_count, position_count
    ) + fading_bias_vector.reshape(attention_group_count, 1, 1, HEAD)
    log_fading_factor = -jnp.exp(
        -jax.nn.softplus(-fading_preactivation) - 0.5
    ) + surplus_forgetting.reshape(attention_group_count, block_count, BLOCK, 1)
    learn_rate = jax.nn.sigmoid(
        by_blocks(step_size_preactivation, attention_group_count, position_count)
    )
    unit_keys = key_rows * lax.rsqrt(jnp.sum(key_rows * key_rows, axis=-1, keepdims=True) + key_eps)
    scaled = key_rows * learn_rate
    removal = unit_keys * learn_rate
    cum_after = jnp.cumsum(log_fading_factor, axis=2)
    before = cum_after - log_fading_factor
    cum_final = cum_after[:, :, -1:, :]
    probe_keys = unit_keys * jnp.exp(before)
    removal_in = removal * jnp.exp(-cum_after)
    scaled_in = scaled * jnp.exp(-cum_after)
    reads_out = read_rows * jnp.exp(cum_after)
    position = jnp.arange(BLOCK)
    strict = position[:, None] > position[None, :]
    up_to = position[:, None] >= position[None, :]
    mutual = jnp.where(
        strict, jnp.einsum("hbtn,hbsn->hbts", probe_keys, removal_in, precision=high), 0.0
    )
    through = jnp.where(
        strict, jnp.einsum("hbtn,hbsn->hbts", probe_keys, scaled_in, precision=high), 0.0
    )
    right_side = jnp.concatenate(
        [probe_keys, jnp.einsum("hbts,hbsn->hbtn", through, value_rows, precision=high)], axis=-1
    )
    solved = unit_lower_solve(mutual, right_side)
    basis_part = solved[..., :HEAD]
    offset = solved[..., HEAD:]
    removal_end = removal * jnp.exp(cum_final - cum_after)
    scaled_end = scaled * jnp.exp(cum_final - cum_after)
    carry_map = jnp.eye(HEAD, dtype=jnp.float32) * jnp.exp(cum_final) - jnp.einsum(
        "hbtk,hbtj->hbkj", basis_part, removal_end, precision=high
    )
    carry_add = jnp.einsum(
        "hbtv,hbtj->hbvj", value_rows, scaled_end, precision=high
    ) - jnp.einsum("hbtv,hbtj->hbvj", offset, removal_end, precision=high)
    summary = (carry_map[:, 0], carry_add[:, 0])
    for block in range(1, block_count):
        summary = compose(summary, (carry_map[:, block], carry_add[:, block]))
    carried = carried_in(summary)
    starts = [carried]
    for block in range(block_count - 1):
        carried = (
            jnp.einsum("hvk,hkj->hvj", carried, carry_map[:, block], precision=high)
            + carry_add[:, block]
        )
        starts.append(carried)
    starts = jnp.stack(starts, axis=1)
    removed = -jnp.einsum("hbtk,hbvk->hbtv", basis_part, starts, precision=high) - offset
    reach_removal = jnp.where(
        up_to, jnp.einsum("hbtn,hbsn->hbts", reads_out, removal_in, precision=high), 0.0
    )
    reach_value = jnp.where(
        up_to, jnp.einsum("hbtn,hbsn->hbts", reads_out, scaled_in, precision=high), 0.0
    )
    outputs = (
        jnp.einsum("hbtk,hbvk->hbtv", reads_out, starts, precision=high)
        + jnp.einsum("hbts,hbsv->hbtv", reach_removal, removed, precision=high)
        + jnp.einsum("hbts,hbsv->hbtv", reach_value, value_rows, precision=high)
    )
    centred = outputs - jnp.mean(outputs, axis=-1, keepdims=True)
    normed_heads = centred * lax.rsqrt(
        jnp.mean(centred * centred, axis=-1, keepdims=True) + group_eps
    )
    normed_heads = normed_heads.transpose(0, 3, 1, 2).reshape(
        attention_group_count * HEAD, position_count
    )
    mixed_out = (
        normed_heads * per_group_scaler[:, None] * attention_result_switch.astype(jnp.float32)
    ).astype(jnp.bfloat16)
    tp_place = lax.axis_index("tp")
    rows = residual_matrix.shape[0]
    partial = jnp.einsum(
        "ct,cd->td", mixed_out, attention_result_matrix, preferred_element_type=jnp.float32
    )

    def rows_of(x, by):
        owner = (tp_place + by) % count_tp
        return lax.dynamic_slice_in_dim(x, owner * rows, rows, 0)

    sent = partial.astype(jnp.bfloat16)
    middle = residual_matrix.astype(jnp.float32) + rows_of(partial, 0)
    for by in range(1, count_tp):
        middle = middle + shifted(rows_of(sent, by), "tp", by).astype(jnp.float32)
    normed = rms_rows(middle, dense_block_scaler)
    depth = switching_matrix.shape[0]

    def column_blocks(x):
        return [x[:, i * depth : (i + 1) * depth] for i in range(x.shape[1] // depth)]

    turned = rolled(normed, ring_place * 2 * depth)
    blocks = column_blocks(turned)
    flipped = jnp.concatenate([blocks[i ^ 1] for i in range(count_sp)], axis=1)
    near = jnp.where(parity == 0, turned, flipped)
    far = paired(jnp.where(parity == 0, flipped, turned))

    def spread(x):
        return jnp.concatenate([x] + [shifted(x, "tp", by) for by in range(1, count_tp)], axis=0)

    def stacked(pieces):
        return jnp.concatenate([x for pair in zip(*pieces) for x in pair], axis=0)

    wide_weight = stacked(wide_pieces)

    def units_of(x):
        both = jnp.dot(x, wide_weight, preferred_element_type=jnp.float32)
        return (jax.nn.silu(both[:, :units]) * both[:, units:]).astype(jnp.bfloat16)

    near_units = units_of(spread(near))
    near_sent = paired(near_units)
    far_units = units_of(spread(far))
    far_sent = paired(far_units)
    down_own = jnp.concatenate(down_pieces[0], axis=1)
    down_other = jnp.concatenate(down_pieces[1], axis=1)

    def summed(own, other):
        product = (
            jnp.dot(own, down_own, preferred_element_type=jnp.float32)
            + jnp.dot(other, down_other, preferred_element_type=jnp.float32)
        ).astype(jnp.bfloat16)
        total = product[:rows].astype(jnp.float32)
        for by in range(1, count_tp):
            total = total + shifted(product[by * rows : (by + 1) * rows], "tp", -by).astype(
                jnp.float32
            )
        return total

    far_sum = paired(summed(far_units, near_sent).astype(jnp.bfloat16)).astype(jnp.float32)
    near_sum = summed(near_units, far_sent)
    even = column_blocks(jnp.where(parity == 0, near_sum, far_sum))
    odd = column_blocks(jnp.where(parity == 0, far_sum, near_sum))
    columns = jnp.concatenate([x for pair in zip(even, odd) for x in pair], axis=1)
    channel_out = rolled(columns, (count_sp // 2 - ring_place) % (count_sp // 2) * 2 * depth)
    return (middle + channel_out).astype(jnp.bfloat16)


LANES = 128
PAIR = 2
MESH = pl.DeviceIdType.MESH
f32, bf16 = jnp.float32, jnp.bfloat16
NN = (((1,), (0,)), ((), ()))
NT = (((1,), (1,)), ((), ()))


def mm(a, b, dims=NN):
    return lax.dot_general(a, b, dims, preferred_element_type=f32)


def split(x):
    top = x.astype(bf16)
    return top, (x - top.astype(f32)).astype(bf16)


def mm3(a, b, dims=NN):
    (ah, al), (bh, bl) = split(a), split(b)
    return mm(ah, bh, dims) + mm(ah, bl, dims) + mm(al, bh, dims)


def mm2(a, b, dims=NN):
    bh, bl = split(b)
    return mm(a, bh, dims) + mm(a, bl, dims)


def grid_of(rows):
    return (
        lax.broadcasted_iota(jnp.int32, (rows, LANES), 0),
        lax.broadcasted_iota(jnp.int32, (rows, LANES), 1),
    )


def heads_apart(x):
    row, col = grid_of(LANES)
    return jnp.where((row < HEAD) == (col < HEAD), jnp.concatenate([x, x], axis=0), 0.0)


def inverses(mutuals):
    row, col = grid_of(LANES)
    eye = jnp.where(row == col, 1.0, 0.0)
    solved = [eye - jnp.where((row % 2 == 0) & (col == row + 1), a, 0.0) for a in mutuals]
    for level in range(1, LANES.bit_length() - 1):
        size = 1 << level
        cross = ((row // size) % 2 == 0) & (col // size == row // size + 1)
        rounded = [s.astype(bf16) for s in solved]
        moved = [
            mm(r, jnp.where(cross, a, 0.0).astype(bf16)).astype(bf16)
            for r, a in zip(rounded, mutuals)
        ]
        solved = [s - mm(m, r) for s, m, r in zip(solved, moved, rounded)]
    rest = [eye - s - mm3(a, s) for a, s in zip(mutuals, solved)]
    return [s + mm(s.astype(bf16), r.astype(bf16)) for s, r in zip(solved, rest)]


def layer_kernel(
    zn,
    resid, query, key, value, fading, step_size, switch, bias, surplus, head_gain, row_gain,
    wo, wg, wu, wd,
    out,
    wo_v, gbuf, ubuf, dbuf,
    solved_s, reach_r, reach_v, reads_s, map_s, add_s, read_map, read_add,
    own_sum, sum_out, sum_in, pair_sum, state_out, state_in, entering,
    mixed, part, kept, core_out, core_in, y_out, y_in, z_out, z_in,
    middle, tokens, hidden,
    local_sem, wz_s, wz_r, wx_s, wx_r, sum_sem, state_sem,
    core_s, core_r, y_s, y_r, z_s, z_r,
    own_s, ring_s, ring_r, ty_s, ty_r, tc_s, tc_r, td_s, td_r,
):
    sp, tp = lax.axis_index("sp"), lax.axis_index("tp")
    z, x = sp // PAIR, sp % PAIR
    t_core = tp + 1 - 2 * (tp % 2)
    t_y = (tp + 2) % 4
    t_both = (t_core + 2) % 4
    rows, width = resid.shape
    positions = query.shape[1]
    blocks = positions // LANES
    pairs = query.shape[0] // LANES
    depth = wg.shape[0]
    taken = gbuf.shape[1] // LANES
    tiles = wg.shape[1] // LANES
    bits = (zn - 1).bit_length()

    def zx(g):
        return sum(((z // (1 << i) + (g >> i)) % 2) * (1 << i) for i in range(bits))

    def at(zz, xx, tt):
        return {"sp": zz * PAIR + xx, "tp": tt}

    def first_tile(zz):
        return (zz * (tiles - taken)) // (zn - 1)

    def remote(src, dst, send, recv, to):
        return pltpu.make_async_remote_copy(
            src_ref=src, dst_ref=dst, send_sem=send, recv_sem=recv, device_id=to, device_id_type=MESH
        )

    x_peer, y_peer, core_peer = at(z, 1 - x, tp), at(z, x, t_y), at(z, x, t_core)

    barrier = pltpu.get_barrier_semaphore()
    peers = [x_peer, y_peer, core_peer] + [at(zx(g), x, tp) for g in range(1, zn)]
    for peer in peers:
        pl.semaphore_signal(barrier, inc=1, device_id=peer, device_id_type=MESH)
    pl.semaphore_wait(barrier, len(peers))

    def wide(ref, zz):
        return ref.at[:, pl.ds(pl.multiple_of(first_tile(zz) * LANES, LANES), taken * LANES)]

    def tall(ref, zz):
        return ref.at[pl.ds(pl.multiple_of(first_tile(zz) * LANES, LANES), taken * LANES), :]

    def slots(place):
        span = pl.ds(pl.multiple_of(place * depth, depth), depth)
        return gbuf.at[span, :], ubuf.at[span, :], dbuf.at[:, span]

    def cut(zz):
        return wide(wg, zz), wide(wu, zz), tall(wd, zz)

    own_copies = [pltpu.make_async_copy(wo, wo_v, local_sem.at[3])] + [
        pltpu.make_async_copy(a, b, local_sem.at[i])
        for i, (a, b) in enumerate(zip(cut(z), slots(sp)))
    ]

    def z_weights(g):
        return [
            remote(a, b, wz_s.at[g, i], wz_r.at[g, i], at(zx(g), x, tp))
            for i, (a, b) in enumerate(zip(cut(zx(g)), slots(sp)))
        ]

    def x_weights(g):
        there = slots(zx(g) * PAIR + x)
        return [
            remote(a, b, wx_s.at[g, i], wx_r.at[g, i], x_peer)
            for i, (a, b) in enumerate(zip(cut(z) if g == 0 else there, there))
        ]

    def start(copies):
        for c in copies:
            c.start()

    def forward(g):
        for c, onward in zip(z_weights(g), x_weights(g)):
            c.wait_recv()
            onward.start()

    far_first = list(range(zn - 1, 0, -1))
    start(own_copies)
    start(x_weights(0))
    start(z_weights(far_first[0]))

    row, col = grid_of(LANES)
    strict, up_to = row < col, row <= col
    row_h, col_h = grid_of(HEAD)
    left = col_h < HEAD

    def first_part(hp, _):
        r0 = pl.multiple_of(hp * LANES, LANES)
        here = pl.ds(r0, LANES)
        keys = key[here, :].astype(f32)
        extra = jnp.concatenate(
            [
                jnp.broadcast_to(surplus[pl.ds(2 * hp + i, 1), :], (HEAD, positions))
                for i in range(2)
            ],
            axis=0,
        )
        pre = fading[here, :].astype(f32) + bias[here, :]
        log_fade = -0.6065306597126334 / (1.0 + jnp.exp(-pre)) + extra
        rate = 1.0 / (1.0 + jnp.exp(-step_size[here, :].astype(f32)))
        unit = jnp.concatenate(
            [
                h * lax.rsqrt(jnp.sum(h * h, axis=0, keepdims=True) + key_eps)
                for h in (keys[:HEAD], keys[HEAD:])
            ],
            axis=0,
        )
        removal, scaled = unit * rate, keys * rate
        reads = query[here, :].astype(f32)
        values = value[here, :]
        ones = jnp.where(up_to, 1.0, 0.0).astype(bf16)
        mutuals, grams, ends, probes = [], [], [], []
        for b in range(blocks):
            lanes = slice(b * LANES, (b + 1) * LANES)
            fade = log_fade[:, lanes]
            f1 = fade.astype(bf16)
            left_over = fade - f1.astype(f32)
            f2 = left_over.astype(bf16)
            f3 = (left_over - f2.astype(f32)).astype(bf16)
            after = mm(f1, ones) + (mm(f2, ones) + mm(f3, ones))
            before = after - fade
            mid, last = after[:, HEAD - 1 : HEAD], after[:, LANES - 1 :]
            shrink = jnp.exp(mid - after)
            probe = unit[:, lanes] * jnp.exp(before - mid)
            read = reads[:, lanes] * jnp.exp(after - mid)
            removal_in, scaled_in = removal[:, lanes] * shrink, scaled[:, lanes] * shrink
            to_mid, to_end = jnp.exp(mid), jnp.exp(last - mid)
            reads_s[hp * blocks + b] = read * to_mid
            probes.append(probe * to_mid)
            ends.append((removal_in * to_end, scaled_in * to_end, jnp.exp(last)))
            none = jnp.zeros((HEAD, LANES), f32)
            for hh in range(2):
                own = slice(hh * HEAD, (hh + 1) * HEAD)
                turned = jnp.concatenate([removal_in[own], scaled_in[own]], axis=0).T
                right = jnp.concatenate(
                    [
                        jnp.concatenate([probe[own], read[own], none, none], axis=1),
                        jnp.concatenate([none, none, probe[own], read[own]], axis=1),
                    ],
                    axis=0,
                )
                gram = mm3(turned, right)
                mutuals.append(jnp.where(strict, gram[:, :LANES], 0.0))
                place = (hp * blocks + b) * 2 + hh
                reach_r[place] = jnp.where(up_to, gram[:, LANES : 2 * LANES], 0.0)
                reach_v[place] = jnp.where(up_to, gram[:, 3 * LANES :], 0.0)
                grams.append(jnp.where(strict, gram[:, 2 * LANES : 3 * LANES], 0.0))
        inverse = inverses(mutuals)
        total = None
        for b in range(blocks):
            lanes = slice(b * LANES, (b + 1) * LANES)
            removal_end, scaled_end, fade_end = ends[b]
            taken_out, added = [], []
            for hh in range(2):
                own = slice(hh * HEAD, (hh + 1) * HEAD)
                vals = values[own, lanes]
                right = jnp.concatenate([probes[b][own], mm2(vals, grams[b * 2 + hh])], axis=0)
                solved = mm3(right, inverse[b * 2 + hh])
                solved_s[(hp * blocks + b) * 2 + hh] = solved
                taken_out.append(mm3(solved, removal_end, NT))
                added.append(mm2(vals, scaled_end, NT))
            both = [jnp.where(left, taken_out[0][i], taken_out[1][i]) for i in (slice(0, HEAD), slice(HEAD, LANES))]
            fade_both = jnp.where(left, fade_end[:HEAD], fade_end[HEAD:])
            carry_map = jnp.where(row_h == col_h % HEAD, fade_both, 0.0) - both[0]
            carry_add = jnp.where(left, added[0], added[1]) - both[1]
            map_s[hp * blocks + b] = carry_map
            add_s[hp * blocks + b] = carry_add
            if total is None:
                total = jnp.concatenate([carry_map, carry_add], axis=0)
            else:
                total = mm3(total, heads_apart(carry_map)) + jnp.concatenate(
                    [jnp.zeros_like(carry_add), carry_add], axis=0
                )
        own_sum[hp] = total
        sum_out[hp] = total.astype(bf16)
        return _

    lax.fori_loop(0, pairs, first_part, 0)

    sum_copy = remote(sum_out, sum_in, sum_sem.at[0], sum_sem.at[1], x_peer)
    sum_copy.start()

    def reading_part(hp, _):
        here = pl.ds(pl.multiple_of(hp * LANES, LANES), LANES)
        for b in range(blocks):
            lanes = slice(b * LANES, (b + 1) * LANES)
            maps, adds = [], []
            reads = reads_s[hp * blocks + b]
            values = value[here, lanes]
            for hh in range(2):
                own = slice(hh * HEAD, (hh + 1) * HEAD)
                place = (hp * blocks + b) * 2 + hh
                gone = mm3(solved_s[place], reach_r[place])
                maps.append(reads[own] - gone[:HEAD])
                adds.append(mm2(values[own], reach_v[place]) - gone[HEAD:])
            read_map[hp * blocks + b] = jnp.concatenate(maps, axis=0)
            read_add[hp * blocks + b] = jnp.concatenate(adds, axis=0)
        return _

    lax.fori_loop(0, pairs, reading_part, 0)
    sum_copy.wait_recv()

    def pair_part(hp, _):
        got, own = sum_in[hp].astype(f32), own_sum[hp]
        first = jnp.where(x == 0, own, got)
        second = jnp.where(x == 0, got, own)
        pair_sum[hp] = mm3(first, heads_apart(second[:HEAD])) + jnp.concatenate(
            [jnp.zeros((HEAD, LANES), f32), second[HEAD:]], axis=0
        )
        return _

    lax.fori_loop(0, pairs, pair_part, 0)

    up_z, down_z = (z + 1) % zn, (z + zn - 1) % zn
    state_copy = remote(state_out, state_in, state_sem.at[0], state_sem.at[1], at(up_z, x, tp))

    @pl.when(z == 0)
    def _():
        state_in[...] = jnp.zeros_like(state_in)

    @pl.when(z > 0)
    def _():
        state_copy.wait_recv()

    def chain_part(hp, _):
        state_out[hp] = (
            mm2(state_in[hp], heads_apart(pair_sum[hp, :HEAD])) + pair_sum[hp, HEAD:]
        ).astype(bf16)
        return _

    lax.fori_loop(0, pairs, chain_part, 0)

    @pl.when(z < zn - 1)
    def _():
        state_copy.start()

    for g in far_first[1:]:
        start(z_weights(g))

    def second_part(hp, _):
        r0 = pl.multiple_of(hp * LANES, LANES)
        here = pl.ds(r0, LANES)
        came = state_in[hp].astype(f32)
        got = sum_in[hp].astype(f32)
        state = jnp.where(x == 0, came, mm3(came, heads_apart(got[:HEAD])) + got[HEAD:])
        for b in range(blocks):
            place = hp * blocks + b
            result = mm3(heads_apart(state), read_map[place]) + read_add[place]
            normed = []
            for h in (result[:HEAD], result[HEAD:]):
                centred = h - jnp.mean(h, axis=0, keepdims=True)
                normed.append(
                    centred * lax.rsqrt(jnp.mean(centred * centred, axis=0, keepdims=True) + group_eps)
                )
            lanes = slice(b * LANES, (b + 1) * LANES)
            done = jnp.concatenate(normed, axis=0) * head_gain[here, :] * switch[here, lanes].astype(f32)
            mixed[lanes, here] = done.T.astype(bf16)
            if b + 1 < blocks:
                state = mm3(state, heads_apart(map_s[place])) + add_s[place]
        return _

    lax.fori_loop(0, pairs, second_part, 0)

    step = 4 * LANES
    own_copies[0].wait()

    def project(i, _):
        cols = pl.ds(pl.multiple_of(i * step, step), step)
        part[0, :, cols] = mm(mixed[...], wo_v[:, cols])
        return _

    lax.fori_loop(0, width // step, project, 0)

    def rows_for(t):
        return pl.ds(pl.multiple_of(t * rows, rows), rows)

    def core_copy(i):
        return remote(core_out.at[i], core_in.at[i], core_s.at[i], core_r.at[i], core_peer)

    def y_copy(i):
        return remote(y_out.at[i], y_in.at[i], y_s.at[i], y_r.at[i], y_peer)

    def send_core(i, buf):
        core_out[i, 0] = part[buf, rows_for(t_core), :].astype(bf16)
        core_out[i, 1] = part[buf, rows_for(t_both), :].astype(bf16)
        core_copy(i).start()

    def send_y(i, buf):
        core_copy(i).wait_recv()
        y_out[i] = (part[buf, rows_for(t_y), :] + core_in[i, 1].astype(f32)).astype(bf16)
        y_copy(i).start()
        kept[i] = part[buf, rows_for(tp), :] + core_in[i, 0].astype(f32)

    send_core(zn, 0)
    send_y(zn, 0)
    forward(far_first[0])
    y_copy(zn).wait_recv()
    middle[...] = resid[...].astype(f32) + (kept[zn] + y_in[zn].astype(f32))
    mid_rows = middle[...]
    scale = lax.rsqrt(jnp.mean(mid_rows * mid_rows, axis=-1, keepdims=True) + norm_eps)
    tokens[z, rows_for(tp), :] = (mid_rows * scale * row_gain[...]).astype(bf16)

    def piece(zz, t):
        return tokens.at[zz, rows_for(t), :]

    def up_copy(zz, sem):
        return remote(piece(zz, tp), piece(zz, tp), sem, ring_r.at[zz], at(up_z, x, tp))

    def down_copy(zz, sem):
        return remote(piece(zz, tp), piece(zz, tp), sem, ring_r.at[zz], at(down_z, x, tp))

    def when(cond, action):
        pl.when(cond)(action)

    def y_token(g):
        return remote(piece(zx(g), tp), piece(zx(g), tp), ty_s.at[g], ty_r.at[g], y_peer)

    def y_token_came(g):
        return remote(piece(zx(g), t_y), piece(zx(g), t_y), ty_s.at[g], ty_r.at[g], y_peer)

    def core_token(g):
        return remote(piece(zx(g), tp), piece(zx(g), tp), tc_s.at[g], tc_r.at[g], core_peer)

    def core_token_came(g):
        return remote(piece(zx(g), t_core), piece(zx(g), t_core), tc_s.at[g], tc_r.at[g], core_peer)

    def both_token(g):
        return remote(piece(zx(g), t_y), piece(zx(g), t_y), td_s.at[g], td_r.at[g], core_peer)

    def both_token_came(g):
        return remote(piece(zx(g), t_both), piece(zx(g), t_both), td_s.at[g], td_r.at[g], core_peer)

    def spread_z(g):
        zz = zx(g)
        if g == 0:
            when(z < zn - 1, lambda: up_copy(zz, own_s.at[0]).start())
            when(z > 0, lambda: down_copy(zz, own_s.at[1]).start())
        else:
            up_copy(zz, ring_s.at[g]).wait_recv()
            when((zz < z) & (z < zn - 1), lambda: up_copy(zz, ring_s.at[g]).start())
            when((zz > z) & (z > 0), lambda: down_copy(zz, ring_s.at[g]).start())
        y_token(g).start()
        core_token(g).start()

    def spread_y(g):
        y_token_came(g).wait_recv()
        both_token(g).start()

    spread_z(0)
    spread_y(0)
    for g in far_first[1:]:
        forward(g)
    for g in range(1, zn):
        spread_z(g)
        spread_y(g)
    for c in own_copies[1:]:
        c.wait()
    for g in range(zn):
        for c in x_weights(g):
            c.wait_recv()

    unit_at = lax.broadcasted_iota(jnp.int32, (1, taken * LANES), 1)
    mine = unit_at >= jnp.where(z == 0, 0, (first_tile(z - 1) + taken - first_tile(z)) * LANES)

    def feed(g, buf):
        core_token_came(g).wait_recv()
        both_token_came(g).wait_recv()
        block = tokens[zx(g)]
        gate = mm(block, gbuf[...])
        up = mm(block, ubuf[...])
        hidden[...] = jnp.where(mine, gate / (1.0 + jnp.exp(-gate)) * up, 0.0).astype(bf16)

        def down(i, _):
            cols = pl.ds(pl.multiple_of(i * step, step), step)
            part[buf, :, cols] = mm(hidden[...], dbuf[:, cols])
            return _

        lax.fori_loop(0, width // step, down, 0)

    def z_copy(g):
        return remote(z_out.at[g], z_in.at[g], z_s.at[g], z_r.at[g], at(zx(g), x, tp))

    def send_z(g):
        y_copy(g).wait_recv()
        if g == 0:
            kept[g] = kept[g] + y_in[g].astype(f32)
        else:
            z_out[g] = (kept[g] + y_in[g].astype(f32)).astype(bf16)
            z_copy(g).start()

    order = list(range(1, zn)) + [0]
    for i, g in enumerate(order):
        feed(g, i % 2)
        send_core(g, i % 2)
        if i >= 1:
            send_y(order[i - 1], (i - 1) % 2)
        if i >= 2:
            send_z(order[i - 2])
    send_y(order[-1], (zn - 1) % 2)
    send_z(order[-2])
    send_z(order[-1])
    total = middle[...] + kept[0]
    for g in range(1, zn):
        z_copy(g).wait_recv()
        total = total + z_in[g].astype(f32)
    out[...] = total.astype(bf16)

    for g in range(1, zn):
        for c in z_weights(g):
            c.wait_send()
        z_copy(g).wait_send()
        zz = zx(g)
        moved_on = ((zz < z) & (z < zn - 1)) | ((zz > z) & (z > 0))
        when(moved_on, up_copy(zz, ring_s.at[g]).wait_send)
    for g in range(zn):
        for c in x_weights(g):
            c.wait_send()
        y_token(g).wait_send()
        core_token(g).wait_send()
        both_token(g).wait_send()
    for i in range(zn + 1):
        core_copy(i).wait_send()
        y_copy(i).wait_send()
    sum_copy.wait_send()
    when(z < zn - 1, state_copy.wait_send)
    when(z < zn - 1, up_copy(z, own_s.at[0]).wait_send)
    when(z > 0, down_copy(z, own_s.at[1]).wait_send)


def fits(mesh, *arrays):
    sp, tp = mesh.shape["sp"], mesh.shape["tp"]
    heads, positions = arrays[8].shape
    units = arrays[12].shape[1]
    zn = sp // PAIR
    return (
        tp == 4
        and sp % PAIR == 0
        and zn > 1
        and zn & (zn - 1) == 0
        and heads % 2 == 0
        and positions % LANES == 0
        and positions == tp * arrays[0].shape[0]
        and units % LANES == 0
        and units // LANES >= zn
        and arrays[12].shape[0] % LANES == 0
        and arrays[0].shape[1] % (4 * LANES) == 0
    )


def fused(
    residual, query, key, value, fading, step_size, switch, bias, surplus, head_gain, out_proj,
    row_gain, gate_up, expand, contract,
):
    zn = lax.axis_size("sp") // PAIR
    rows, width = residual.shape
    channels, positions = query.shape
    pairs, blocks = channels // LANES, positions // LANES
    many = pairs * blocks
    taken = -(-(gate_up.shape[1] // LANES) // zn) * LANES
    square = (LANES, LANES)
    half = (HEAD, LANES)
    vmem, dma = pltpu.VMEM, pltpu.SemaphoreType.DMA
    scratch = [
        vmem(out_proj.shape, bf16),
        vmem((width, taken), bf16),
        vmem((width, taken), bf16),
        vmem((taken, width), bf16),
        vmem((2 * many, *square), f32),
        vmem((2 * many, *square), f32),
        vmem((2 * many, *square), f32),
        vmem((many, *square), f32),
        vmem((many, *half), f32),
        vmem((many, *half), f32),
        vmem((many, *square), f32),
        vmem((many, *square), f32),
        vmem((pairs, *square), f32),
        vmem((pairs, *square), bf16),
        vmem((pairs, *square), bf16),
        vmem((pairs, *square), f32),
        vmem((pairs, *half), bf16),
        vmem((pairs, *half), bf16),
        vmem((pairs, *half), f32),
        vmem((positions, channels), bf16),
        vmem((2, positions, width), f32),
        vmem((zn + 1, rows, width), f32),
        vmem((zn + 1, 2, rows, width), bf16),
        vmem((zn + 1, 2, rows, width), bf16),
        vmem((zn + 1, rows, width), bf16),
        vmem((zn + 1, rows, width), bf16),
        vmem((zn, rows, width), bf16),
        vmem((zn, rows, width), bf16),
        vmem((rows, width), f32),
        vmem((zn, positions, width), bf16),
        vmem((positions, taken), bf16),
        dma((4,)),
        dma((zn, 3)), dma((zn, 3)), dma((zn, 3)), dma((zn, 3)),
        dma((2,)), dma((2,)),
        dma((zn + 1,)), dma((zn + 1,)), dma((zn + 1,)), dma((zn + 1,)), dma((zn,)), dma((zn,)),
        dma((2,)), dma((zn,)), dma((zn,)),
        dma((zn,)), dma((zn,)), dma((zn,)), dma((zn,)), dma((zn,)), dma((zn,)),
    ]
    inside = pl.BlockSpec(memory_space=pltpu.VMEM)
    outside = pl.BlockSpec(memory_space=pl.ANY)
    return pl.pallas_call(
        functools.partial(layer_kernel, zn),
        out_shape=jax.ShapeDtypeStruct((rows, width), bf16),
        in_specs=[inside] * 11 + [outside] * 4,
        out_specs=inside,
        scratch_shapes=scratch,
        compiler_params=pltpu.CompilerParams(
            collective_id=0, has_side_effects=True, vmem_limit_bytes=60 << 20
        ),
        name="layer",
    )(
        residual, query, key, value, fading, step_size, switch, bias[:, None], surplus,
        head_gain[:, None], row_gain[None, :], out_proj, gate_up, expand, contract,
    )


def solution(mesh):
    placed = (
        P(("sp", "tp"), None),
        P("tp", "sp"),
        P("tp", "sp"),
        P("tp", "sp"),
        P("tp", "sp"),
        P("tp", "sp"),
        P("tp", "sp"),
        P("tp"),
        P("tp", "sp"),
        P("tp"),
        P("tp", None),
        P(),
        P("sp", "tp"),
        P("sp", "tp"),
        P("tp", "sp"),
    )

    def layer(*arrays):
        return (fused if fits(mesh, *arrays) else local)(*arrays)


    return jax.shard_map(
        layer, mesh=mesh, in_specs=placed, out_specs=P(("sp", "tp"), None), check_vma=False
    )
```

```python
import functools
import jax
import jax.numpy as jnp
from jax import lax
from jax.experimental import pallas as pl
from jax.experimental.pallas import tpu as pltpu
from jax.sharding import PartitionSpec as P

HEAD = 64
BLOCK = 64


norm_eps = 1e-06
group_eps = 0.00064
key_eps = 1e-06
highest = lax.Precision.HIGHEST
high = lax.Precision.HIGH


def shifted(x, axis, by):
    n = lax.axis_size(axis)
    return lax.ppermute(x, axis, [(i, (i + by) % n) for i in range(n)])


def paired(x):
    n = lax.axis_size("sp")
    return lax.ppermute(x, "sp", [(i, i ^ 1) for i in range(n)])


def around(first, second):
    n = lax.axis_size("sp")
    ring = n // 2
    half = ring // 2

    def hop(x, by):
        return lax.ppermute(x, "sp", [(i, (i + 2 * by) % n) for i in range(n)])

    out = [[None] * ring, [None] * ring]
    for place, piece in enumerate((first, second)):
        out[place][0] = piece
        up = down = piece
        for step in range(1, half):
            up = hop(up, 1)
            down = hop(down, -1)
            out[place][ring - step] = up
            out[place][step] = down
        if ring > 1:
            out[place][half] = hop(up, 1) if place == 0 else hop(down, -1)
    return out


def rolled(x, by):
    return lax.dynamic_slice_in_dim(jnp.concatenate([x, x], axis=1), by, x.shape[1], 1)


def carried_in(summary):
    n = lax.axis_size("sp")
    carry_map, carry_add = summary
    both = jnp.concatenate([carry_map, carry_add], axis=1).astype(jnp.bfloat16)
    width = carry_map.shape[1]
    state = jnp.zeros_like(carry_add)
    for back in range(n - 1, 0, -1):
        came = lax.ppermute(both, "sp", [(i, i + back) for i in range(n - back)])
        came = came.astype(jnp.float32)
        state = (
            jnp.einsum("hvk,hkj->hvj", state, came[:, :width], precision=high)
            + came[:, width:]
        )
    return state


def by_blocks(source, attention_group_count, position_count):
    return (
        source.astype(jnp.float32)
        .reshape(attention_group_count, HEAD, position_count // BLOCK, BLOCK)
        .transpose(0, 2, 3, 1)
    )


def compose(earlier, latter):
    return (
        jnp.einsum("...ij,...jk->...ik", earlier[0], latter[0], precision=high),
        jnp.einsum("...ij,...jk->...ik", earlier[1], latter[0], precision=high) + latter[1],
    )


def unit_lower_solve(mutual, right_side):
    power = -mutual
    solved = right_side
    for level in range((BLOCK - 1).bit_length()):
        solved = solved + jnp.einsum("hbts,hbsn->hbtn", power, solved, precision=highest)
        if level + 1 < (BLOCK - 1).bit_length():
            power = jnp.einsum("hbts,hbsu->hbtu", power, power, precision=highest)
    return solved


def rms_rows(middle, dense_block_scaler):
    scale_rows = lax.rsqrt(jnp.mean(middle * middle, axis=-1, keepdims=True) + norm_eps)
    return (middle * scale_rows * dense_block_scaler).astype(jnp.bfloat16)


def local(
    residual_matrix,
    query_vectors,
    lookup_vectors,
    payload_vectors,
    fading_dependent_term,
    step_size_preactivation,
    attention_result_switch,
    fading_bias_vector,
    surplus_forgetting,
    per_group_scaler,
    attention_result_matrix,
    dense_block_scaler,
    switching_matrix,
    expanding_matrix,
    contracting_matrix,
):
    count_sp, count_tp = lax.axis_size("sp"), lax.axis_size("tp")
    parity = lax.axis_index("sp") % 2
    ring_place = lax.axis_index("sp") // 2
    units = switching_matrix.shape[1] // 2

    def part(x, which, axis):
        return lax.dynamic_slice_in_dim(x, which * units, units, axis)

    def gate_up(which):
        return jnp.concatenate(
            [part(switching_matrix, which, 1), part(expanding_matrix, which, 1)], axis=1
        )

    wide_pieces = around(gate_up(parity), paired(gate_up(1 - parity)))
    down_pieces = around(
        part(contracting_matrix, parity, 0), part(contracting_matrix, 1 - parity, 0)
    )
    attention_group_count = surplus_forgetting.shape[0]
    position_count = surplus_forgetting.shape[1]
    block_count = position_count // BLOCK
    read_rows = by_blocks(query_vectors, attention_group_count, position_count)
    key_rows = by_blocks(lookup_vectors, attention_group_count, position_count)
    value_rows = by_blocks(payload_vectors, attention_group_count, position_count)
    fading_preactivation = by_blocks(
        fading_dependent_term, attention_group_count, position_count
    ) + fading_bias_vector.reshape(attention_group_count, 1, 1, HEAD)
    log_fading_factor = -jnp.exp(
        -jax.nn.softplus(-fading_preactivation) - 0.5
    ) + surplus_forgetting.reshape(attention_group_count, block_count, BLOCK, 1)
    learn_rate = jax.nn.sigmoid(
        by_blocks(step_size_preactivation, attention_group_count, position_count)
    )
    unit_keys = key_rows * lax.rsqrt(jnp.sum(key_rows * key_rows, axis=-1, keepdims=True) + key_eps)
    scaled = key_rows * learn_rate
    removal = unit_keys * learn_rate
    cum_after = jnp.cumsum(log_fading_factor, axis=2)
    before = cum_after - log_fading_factor
    cum_final = cum_after[:, :, -1:, :]
    probe_keys = unit_keys * jnp.exp(before)
    removal_in = removal * jnp.exp(-cum_after)
    scaled_in = scaled * jnp.exp(-cum_after)
    reads_out = read_rows * jnp.exp(cum_after)
    position = jnp.arange(BLOCK)
    strict = position[:, None] > position[None, :]
    up_to = position[:, None] >= position[None, :]
    mutual = jnp.where(
        strict, jnp.einsum("hbtn,hbsn->hbts", probe_keys, removal_in, precision=high), 0.0
    )
    through = jnp.where(
        strict, jnp.einsum("hbtn,hbsn->hbts", probe_keys, scaled_in, precision=high), 0.0
    )
    right_side = jnp.concatenate(
        [probe_keys, jnp.einsum("hbts,hbsn->hbtn", through, value_rows, precision=high)], axis=-1
    )
    solved = unit_lower_solve(mutual, right_side)
    basis_part = solved[..., :HEAD]
    offset = solved[..., HEAD:]
    removal_end = removal * jnp.exp(cum_final - cum_after)
    scaled_end = scaled * jnp.exp(cum_final - cum_after)
    carry_map = jnp.eye(HEAD, dtype=jnp.float32) * jnp.exp(cum_final) - jnp.einsum(
        "hbtk,hbtj->hbkj", basis_part, removal_end, precision=high
    )
    carry_add = jnp.einsum(
        "hbtv,hbtj->hbvj", value_rows, scaled_end, precision=high
    ) - jnp.einsum("hbtv,hbtj->hbvj", offset, removal_end, precision=high)
    summary = (carry_map[:, 0], carry_add[:, 0])
    for block in range(1, block_count):
        summary = compose(summary, (carry_map[:, block], carry_add[:, block]))
    carried = carried_in(summary)
    starts = [carried]
    for block in range(block_count - 1):
        carried = (
            jnp.einsum("hvk,hkj->hvj", carried, carry_map[:, block], precision=high)
            + carry_add[:, block]
        )
        starts.append(carried)
    starts = jnp.stack(starts, axis=1)
    removed = -jnp.einsum("hbtk,hbvk->hbtv", basis_part, starts, precision=high) - offset
    reach_removal = jnp.where(
        up_to, jnp.einsum("hbtn,hbsn->hbts", reads_out, removal_in, precision=high), 0.0
    )
    reach_value = jnp.where(
        up_to, jnp.einsum("hbtn,hbsn->hbts", reads_out, scaled_in, precision=high), 0.0
    )
    outputs = (
        jnp.einsum("hbtk,hbvk->hbtv", reads_out, starts, precision=high)
        + jnp.einsum("hbts,hbsv->hbtv", reach_removal, removed, precision=high)
        + jnp.einsum("hbts,hbsv->hbtv", reach_value, value_rows, precision=high)
    )
    centred = outputs - jnp.mean(outputs, axis=-1, keepdims=True)
    normed_heads = centred * lax.rsqrt(
        jnp.mean(centred * centred, axis=-1, keepdims=True) + group_eps
    )
    normed_heads = normed_heads.transpose(0, 3, 1, 2).reshape(
        attention_group_count * HEAD, position_count
    )
    mixed_out = (
        normed_heads * per_group_scaler[:, None] * attention_result_switch.astype(jnp.float32)
    ).astype(jnp.bfloat16)
    tp_place = lax.axis_index("tp")
    rows = residual_matrix.shape[0]
    partial = jnp.einsum(
        "ct,cd->td", mixed_out, attention_result_matrix, preferred_element_type=jnp.float32
    )

    def rows_of(x, by):
        owner = (tp_place + by) % count_tp
        return lax.dynamic_slice_in_dim(x, owner * rows, rows, 0)

    sent = partial.astype(jnp.bfloat16)
    middle = residual_matrix.astype(jnp.float32) + rows_of(partial, 0)
    for by in range(1, count_tp):
        middle = middle + shifted(rows_of(sent, by), "tp", by).astype(jnp.float32)
    normed = rms_rows(middle, dense_block_scaler)
    depth = switching_matrix.shape[0]

    def column_blocks(x):
        return [x[:, i * depth : (i + 1) * depth] for i in range(x.shape[1] // depth)]

    turned = rolled(normed, ring_place * 2 * depth)
    blocks = column_blocks(turned)
    flipped = jnp.concatenate([blocks[i ^ 1] for i in range(count_sp)], axis=1)
    near = jnp.where(parity == 0, turned, flipped)
    far = paired(jnp.where(parity == 0, flipped, turned))

    def spread(x):
        return jnp.concatenate([x] + [shifted(x, "tp", by) for by in range(1, count_tp)], axis=0)

    def stacked(pieces):
        return jnp.concatenate([x for pair in zip(*pieces) for x in pair], axis=0)

    wide_weight = stacked(wide_pieces)

    def units_of(x):
        both = jnp.dot(x, wide_weight, preferred_element_type=jnp.float32)
        return (jax.nn.silu(both[:, :units]) * both[:, units:]).astype(jnp.bfloat16)

    near_units = units_of(spread(near))
    near_sent = paired(near_units)
    far_units = units_of(spread(far))
    far_sent = paired(far_units)
    down_own = jnp.concatenate(down_pieces[0], axis=1)
    down_other = jnp.concatenate(down_pieces[1], axis=1)

    def summed(own, other):
        product = (
            jnp.dot(own, down_own, preferred_element_type=jnp.float32)
            + jnp.dot(other, down_other, preferred_element_type=jnp.float32)
        ).astype(jnp.bfloat16)
        total = product[:rows].astype(jnp.float32)
        for by in range(1, count_tp):
            total = total + shifted(product[by * rows : (by + 1) * rows], "tp", -by).astype(
                jnp.float32
            )
        return total

    far_sum = paired(summed(far_units, near_sent).astype(jnp.bfloat16)).astype(jnp.float32)
    near_sum = summed(near_units, far_sent)
    even = column_blocks(jnp.where(parity == 0, near_sum, far_sum))
    odd = column_blocks(jnp.where(parity == 0, far_sum, near_sum))
    columns = jnp.concatenate([x for pair in zip(even, odd) for x in pair], axis=1)
    channel_out = rolled(columns, (count_sp // 2 - ring_place) % (count_sp // 2) * 2 * depth)
    return (middle + channel_out).astype(jnp.bfloat16)


LANES = 128
PAIR = 2
MESH = pl.DeviceIdType.MESH
f32, bf16 = jnp.float32, jnp.bfloat16
NN = (((1,), (0,)), ((), ()))
NT = (((1,), (1,)), ((), ()))


def mm(a, b, dims=NN):
    return lax.dot_general(a, b, dims, preferred_element_type=f32)


def split(x):
    top = x.astype(bf16)
    return top, (x - top.astype(f32)).astype(bf16)


def mm3(a, b, dims=NN):
    (ah, al), (bh, bl) = split(a), split(b)
    return mm(ah, bh, dims) + mm(ah, bl, dims) + mm(al, bh, dims)


def mm2(a, b, dims=NN):
    bh, bl = split(b)
    return mm(a, bh, dims) + mm(a, bl, dims)


def grid_of(rows):
    return (
        lax.broadcasted_iota(jnp.int32, (rows, LANES), 0),
        lax.broadcasted_iota(jnp.int32, (rows, LANES), 1),
    )


def heads_apart(x):
    row, col = grid_of(LANES)
    return jnp.where((row < HEAD) == (col < HEAD), jnp.concatenate([x, x], axis=0), 0.0)


def inverses(mutuals):
    row, col = grid_of(LANES)
    eye = jnp.where(row == col, 1.0, 0.0)
    solved = [eye - jnp.where((row % 2 == 0) & (col == row + 1), a, 0.0) for a in mutuals]
    for level in range(1, LANES.bit_length() - 1):
        size = 1 << level
        cross = ((row // size) % 2 == 0) & (col // size == row // size + 1)
        rounded = [s.astype(bf16) for s in solved]
        moved = [
            mm(r, jnp.where(cross, a, 0.0).astype(bf16)).astype(bf16)
            for r, a in zip(rounded, mutuals)
        ]
        solved = [s - mm(m, r) for s, m, r in zip(solved, moved, rounded)]
    rest = [eye - s - mm3(a, s) for a, s in zip(mutuals, solved)]
    return [s + mm(s.astype(bf16), r.astype(bf16)) for s, r in zip(solved, rest)]


def layer_kernel(
    zn,
    resid, query, key, value, fading, step_size, switch, bias, surplus, head_gain, row_gain,
    wo, wg, wu, wd,
    out,
    wo_v, gbuf, ubuf, dbuf,
    solved_s, reach_r, reach_v, reads_s, map_s, add_s, read_map, read_add,
    own_sum, sum_out, sum_in, pair_sum, state_out, state_in, entering,
    mixed, part, kept, core_out, core_in, y_out, y_in, z_out, z_in,
    middle, tokens, hidden,
    local_sem, wz_s, wz_r, wx_s, wx_r, sum_sem, state_sem,
    core_s, core_r, y_s, y_r, z_s, z_r,
    own_s, ring_s, ring_r, ty_s, ty_r, tc_s, tc_r, td_s, td_r,
):
    sp, tp = lax.axis_index("sp"), lax.axis_index("tp")
    z, x = sp // PAIR, sp % PAIR
    t_core = tp + 1 - 2 * (tp % 2)
    t_y = (tp + 2) % 4
    t_both = (t_core + 2) % 4
    rows, width = resid.shape
    positions = query.shape[1]
    blocks = positions // LANES
    pairs = query.shape[0] // LANES
    depth = wg.shape[0]
    taken = gbuf.shape[1] // LANES
    tiles = wg.shape[1] // LANES
    bits = (zn - 1).bit_length()

    own_group = 0

    def is_own(g):
        return isinstance(g, int) and g == own_group

    def zx(g):
        return sum(((z // (1 << i) + g // (1 << i)) % 2) * (1 << i) for i in range(bits))

    def at(zz, xx, tt):
        return {"sp": zz * PAIR + xx, "tp": tt}

    def first_tile(zz):
        return (zz * (tiles - taken)) // (zn - 1)

    def remote(src, dst, send, recv, to):
        return pltpu.make_async_remote_copy(
            src_ref=src, dst_ref=dst, send_sem=send, recv_sem=recv, device_id=to, device_id_type=MESH
        )

    x_peer, y_peer, core_peer = at(z, 1 - x, tp), at(z, x, t_y), at(z, x, t_core)

    barrier = pltpu.get_barrier_semaphore()
    peers = [x_peer, y_peer, core_peer] + [at(zx(g), x, tp) for g in range(1, zn)]
    for peer in peers:
        pl.semaphore_signal(barrier, inc=1, device_id=peer, device_id_type=MESH)
    pl.semaphore_wait(barrier, len(peers))

    def wide(ref, zz):
        return ref.at[:, pl.ds(pl.multiple_of(first_tile(zz) * LANES, LANES), taken * LANES)]

    def tall(ref, zz):
        return ref.at[pl.ds(pl.multiple_of(first_tile(zz) * LANES, LANES), taken * LANES), :]

    def slots(place):
        span = pl.ds(pl.multiple_of(place * depth, depth), depth)
        return gbuf.at[span, :], ubuf.at[span, :], dbuf.at[:, span]

    def cut(zz):
        return wide(wg, zz), wide(wu, zz), tall(wd, zz)

    own_copies = [pltpu.make_async_copy(wo, wo_v, local_sem.at[3])] + [
        pltpu.make_async_copy(a, b, local_sem.at[i])
        for i, (a, b) in enumerate(zip(cut(z), slots(sp)))
    ]

    def z_weights(g):
        return [
            remote(a, b, wz_s.at[g, i], wz_r.at[g, i], at(zx(g), x, tp))
            for i, (a, b) in enumerate(zip(cut(zx(g)), slots(sp)))
        ]

    def x_weights(g):
        there = slots(zx(g) * PAIR + x)
        return [
            remote(a, b, wx_s.at[g, i], wx_r.at[g, i], x_peer)
            for i, (a, b) in enumerate(zip(cut(z) if is_own(g) else there, there))
        ]

    def column(ref, hp):
        return jnp.broadcast_to(ref[pl.ds(hp, 1), :], (LANES, LANES)).T

    def start(copies):
        for c in copies:
            c.start()

    def start_up(g, which):
        pl.when(zx(g) > z)(lambda: start(z_weights(g)[which]))

    def start_down(g, which):
        pl.when(zx(g) < z)(lambda: start(z_weights(g)[which]))

    def forward(g, which):
        for c, onward in zip(z_weights(g)[which], x_weights(g)[which]):
            c.wait_recv()
            onward.start()

    inner = ((z + 1) // 2) % 2
    tail = list(range(4, zn))
    arrive = [3 - inner, 1 + 2 * inner, 2 - inner] + tail if zn >= 4 else [1]
    pieces = [1, 2 + inner, 3 - inner] + tail if zn >= 4 else [1]
    every, wide_two, tall_one = slice(0, 3), slice(0, 2), slice(2, 3)

    far_first = list(range(zn - 1, 0, -1))
    start(own_copies)
    start(x_weights(0))
    for g in far_first:
        start_down(g, every)

    @pl.when(z == 0)
    def _():
        for g in far_first[:-1]:
            start(z_weights(g)[every if g > 2 else wide_two])


    row, col = grid_of(LANES)
    strict, up_to = row < col, row <= col
    row_h, col_h = grid_of(HEAD)
    left = col_h < HEAD

    def prepared(hp, mutuals, grams):
        r0 = pl.multiple_of(hp * LANES, LANES)
        here = pl.ds(r0, LANES)
        keys = key[here, :].astype(f32)
        extra = jnp.concatenate(
            [
                jnp.broadcast_to(surplus[pl.ds(2 * hp + i, 1), :], (HEAD, positions))
                for i in range(2)
            ],
            axis=0,
        )
        pre = fading[here, :].astype(f32) + jnp.tile(column(bias, hp), (1, blocks))
        log_fade = -0.6065306597126334 / (1.0 + jnp.exp(-pre)) + extra
        rate = 1.0 / (1.0 + jnp.exp(-step_size[here, :].astype(f32)))
        unit = jnp.concatenate(
            [
                h * lax.rsqrt(jnp.sum(h * h, axis=0, keepdims=True) + key_eps)
                for h in (keys[:HEAD], keys[HEAD:])
            ],
            axis=0,
        )
        removal, scaled = unit * rate, keys * rate
        reads = query[here, :].astype(f32)
        ones = jnp.where(up_to, 1.0, 0.0).astype(bf16)
        ends, probes = [], []
        for b in range(blocks):
            lanes = slice(b * LANES, (b + 1) * LANES)
            fade = log_fade[:, lanes]
            f1 = fade.astype(bf16)
            left_over = fade - f1.astype(f32)
            f2 = left_over.astype(bf16)
            f3 = (left_over - f2.astype(f32)).astype(bf16)
            after = mm(f1, ones) + (mm(f2, ones) + mm(f3, ones))
            before = after - fade
            mid, last = after[:, HEAD - 1 : HEAD], after[:, LANES - 1 :]
            shrink = jnp.exp(mid - after)
            probe = unit[:, lanes] * jnp.exp(before - mid)
            read = reads[:, lanes] * jnp.exp(after - mid)
            removal_in, scaled_in = removal[:, lanes] * shrink, scaled[:, lanes] * shrink
            to_mid, to_end = jnp.exp(mid), jnp.exp(last - mid)
            reads_s[hp * blocks + b] = read * to_mid
            probes.append(probe * to_mid)
            ends.append((removal_in * to_end, scaled_in * to_end, jnp.exp(last)))
            none = jnp.zeros((HEAD, LANES), f32)
            for hh in range(2):
                own = slice(hh * HEAD, (hh + 1) * HEAD)
                turned = jnp.concatenate([removal_in[own], scaled_in[own]], axis=0).T
                right = jnp.concatenate(
                    [
                        jnp.concatenate([probe[own], read[own], none, none], axis=1),
                        jnp.concatenate([none, none, probe[own], read[own]], axis=1),
                    ],
                    axis=0,
                )
                gram = mm3(turned, right)
                mutuals.append(jnp.where(strict, gram[:, :LANES], 0.0))
                place = (hp * blocks + b) * 2 + hh
                reach_r[place] = jnp.where(up_to, gram[:, LANES : 2 * LANES], 0.0)
                reach_v[place] = jnp.where(up_to, gram[:, 3 * LANES :], 0.0)
                grams.append(jnp.where(strict, gram[:, 2 * LANES : 3 * LANES], 0.0))
        return ends, probes

    def summed(hp, ends, probes, inverse, grams):
        values = value[pl.ds(pl.multiple_of(hp * LANES, LANES), LANES), :]
        total = None
        for b in range(blocks):
            lanes = slice(b * LANES, (b + 1) * LANES)
            removal_end, scaled_end, fade_end = ends[b]
            taken_out, added = [], []
            for hh in range(2):
                own = slice(hh * HEAD, (hh + 1) * HEAD)
                vals = values[own, lanes]
                right = jnp.concatenate([probes[b][own], mm2(vals, grams[b * 2 + hh])], axis=0)
                solved = mm3(right, inverse[b * 2 + hh])
                solved_s[(hp * blocks + b) * 2 + hh] = solved
                taken_out.append(mm3(solved, removal_end, NT))
                added.append(mm2(vals, scaled_end, NT))
            both = [
                jnp.where(left, taken_out[0][i], taken_out[1][i])
                for i in (slice(0, HEAD), slice(HEAD, LANES))
            ]
            fade_both = jnp.where(left, fade_end[:HEAD], fade_end[HEAD:])
            carry_map = jnp.where(row_h == col_h % HEAD, fade_both, 0.0) - both[0]
            carry_add = jnp.where(left, added[0], added[1]) - both[1]
            map_s[hp * blocks + b] = carry_map
            add_s[hp * blocks + b] = carry_add
            if total is None:
                total = jnp.concatenate([carry_map, carry_add], axis=0)
            else:
                total = mm3(total, heads_apart(carry_map)) + jnp.concatenate(
                    [jnp.zeros_like(carry_add), carry_add], axis=0
                )
        own_sum[hp] = total
        sum_out[hp] = total.astype(bf16)

    together = 2 if pairs % 2 == 0 else 1

    def first_part(i, _):
        mutuals, grams, ready = [], [], []
        for j in range(together):
            ready.append(prepared(i * together + j, mutuals, grams))
        inverse = inverses(mutuals)
        for j in range(together):
            span = slice(j * 2 * blocks, (j + 1) * 2 * blocks)
            summed(i * together + j, *ready[j], inverse[span], grams[span])
        return _

    lax.fori_loop(0, pairs // together, first_part, 0)

    sum_copy = remote(sum_out, sum_in, sum_sem.at[0], sum_sem.at[1], x_peer)
    sum_copy.start()

    def reading_part(hp, _):
        here = pl.ds(pl.multiple_of(hp * LANES, LANES), LANES)
        for b in range(blocks):
            lanes = slice(b * LANES, (b + 1) * LANES)
            maps, adds = [], []
            reads = reads_s[hp * blocks + b]
            values = value[here, lanes]
            for hh in range(2):
                own = slice(hh * HEAD, (hh + 1) * HEAD)
                place = (hp * blocks + b) * 2 + hh
                gone = mm3(solved_s[place], reach_r[place])
                maps.append(reads[own] - gone[:HEAD])
                adds.append(mm2(values[own], reach_v[place]) - gone[HEAD:])
            read_map[hp * blocks + b] = jnp.concatenate(maps, axis=0)
            read_add[hp * blocks + b] = jnp.concatenate(adds, axis=0)
        return _

    lax.fori_loop(0, pairs, reading_part, 0)
    sum_copy.wait_recv()

    def pair_part(hp, _):
        got, own = sum_in[hp].astype(f32), own_sum[hp]
        first = jnp.where(x == 0, own, got)
        second = jnp.where(x == 0, got, own)
        pair_sum[hp] = mm3(first, heads_apart(second[:HEAD])) + jnp.concatenate(
            [jnp.zeros((HEAD, LANES), f32), second[HEAD:]], axis=0
        )
        return _

    lax.fori_loop(0, pairs, pair_part, 0)

    up_z, down_z = (z + 1) % zn, (z + zn - 1) % zn
    state_copy = remote(state_out, state_in, state_sem.at[0], state_sem.at[1], at(up_z, x, tp))

    @pl.when(z == 0)
    def _():
        state_in[...] = jnp.zeros_like(state_in)

    @pl.when(z > 0)
    def _():
        state_copy.wait_recv()

    def chain_part(hp, _):
        state_out[hp] = (
            mm2(state_in[hp], heads_apart(pair_sum[hp, :HEAD])) + pair_sum[hp, HEAD:]
        ).astype(bf16)
        return _

    lax.fori_loop(0, pairs, chain_part, 0)

    @pl.when(z < zn - 1)
    def _():
        state_copy.start()

    @pl.when(z == 0)
    def _():
        start(z_weights(1)[wide_two])
        if zn > 2:
            start(z_weights(2)[tall_one])

    @pl.when(z > 0)
    def _():
        for g in [1] + far_first[:-1]:
            start_up(g, every)


    def second_part(hp, _):
        r0 = pl.multiple_of(hp * LANES, LANES)
        here = pl.ds(r0, LANES)
        came = state_in[hp].astype(f32)
        gain = column(head_gain, hp)
        got = sum_in[hp].astype(f32)
        state = jnp.where(x == 0, came, mm3(came, heads_apart(got[:HEAD])) + got[HEAD:])
        for b in range(blocks):
            place = hp * blocks + b
            result = mm3(heads_apart(state), read_map[place]) + read_add[place]
            normed = []
            for h in (result[:HEAD], result[HEAD:]):
                centred = h - jnp.mean(h, axis=0, keepdims=True)
                normed.append(
                    centred * lax.rsqrt(jnp.mean(centred * centred, axis=0, keepdims=True) + group_eps)
                )
            lanes = slice(b * LANES, (b + 1) * LANES)
            done = jnp.concatenate(normed, axis=0) * gain * switch[here, lanes].astype(f32)
            mixed[lanes, here] = done.T.astype(bf16)
            if b + 1 < blocks:
                state = mm3(state, heads_apart(map_s[place])) + add_s[place]
        return _

    lax.fori_loop(0, pairs, second_part, 0)

    step = 4 * LANES
    own_copies[0].wait()

    def project(i, _):
        cols = pl.ds(pl.multiple_of(i * step, step), step)
        part[0, :, cols] = mm(mixed[...], wo_v[:, cols])
        return _

    lax.fori_loop(0, width // step, project, 0)

    def rows_for(t):
        return pl.ds(pl.multiple_of(t * rows, rows), rows)

    def core_copy(i):
        return remote(core_out.at[i], core_in.at[i], core_s.at[i], core_r.at[i], core_peer)

    def y_copy(i):
        return remote(y_out.at[i], y_in.at[i], y_s.at[i], y_r.at[i], y_peer)

    def send_core(i, buf):
        core_out[i, 0] = part[buf, rows_for(t_core), :].astype(bf16)
        core_out[i, 1] = part[buf, rows_for(t_both), :].astype(bf16)
        core_copy(i).start()

    def send_y(i, buf):
        core_copy(i).wait_recv()
        y_out[i] = (part[buf, rows_for(t_y), :] + core_in[i, 1].astype(f32)).astype(bf16)
        y_copy(i).start()
        kept[i] = part[buf, rows_for(tp), :] + core_in[i, 0].astype(f32)

    send_core(zn, 0)
    send_y(zn, 0)
    forward(arrive[0], wide_two)
    y_copy(zn).wait_recv()
    middle[...] = resid[...].astype(f32) + (kept[zn] + y_in[zn].astype(f32))
    mid_rows = middle[...]
    scale = lax.rsqrt(jnp.mean(mid_rows * mid_rows, axis=-1, keepdims=True) + norm_eps)
    tokens[z, rows_for(tp), :] = (mid_rows * scale * row_gain[...]).astype(bf16)

    def piece(zz, t):
        return tokens.at[zz, rows_for(t), :]

    def up_copy(zz, sem):
        return remote(piece(zz, tp), piece(zz, tp), sem, ring_r.at[zz], at(up_z, x, tp))

    def down_copy(zz, sem):
        return remote(piece(zz, tp), piece(zz, tp), sem, ring_r.at[zz], at(down_z, x, tp))

    def when(cond, action):
        pl.when(cond)(action)

    def y_token(g):
        return remote(piece(zx(g), tp), piece(zx(g), tp), ty_s.at[g], ty_r.at[g], y_peer)

    def y_token_came(g):
        return remote(piece(zx(g), t_y), piece(zx(g), t_y), ty_s.at[g], ty_r.at[g], y_peer)

    def core_token(g):
        return remote(piece(zx(g), tp), piece(zx(g), tp), tc_s.at[g], tc_r.at[g], core_peer)

    def core_token_came(g):
        return remote(piece(zx(g), t_core), piece(zx(g), t_core), tc_s.at[g], tc_r.at[g], core_peer)

    def both_token(g):
        return remote(piece(zx(g), t_y), piece(zx(g), t_y), td_s.at[g], td_r.at[g], core_peer)

    def both_token_came(g):
        return remote(piece(zx(g), t_both), piece(zx(g), t_both), td_s.at[g], td_r.at[g], core_peer)

    def spread_z(g):
        zz = zx(g)
        if is_own(g):
            when(z < zn - 1, lambda: up_copy(zz, own_s.at[0]).start())
            when(z > 0, lambda: down_copy(zz, own_s.at[1]).start())
        else:
            up_copy(zz, ring_s.at[g]).wait_recv()
            when((zz < z) & (z < zn - 1), lambda: up_copy(zz, ring_s.at[g]).start())
            when((zz > z) & (z > 0), lambda: down_copy(zz, ring_s.at[g]).start())
        y_token(g).start()
        core_token(g).start()

    def spread_y(g):
        y_token_came(g).wait_recv()
        both_token(g).start()

    spread_z(own_group)
    pl.when(z == 0)(lambda: start(z_weights(1)[tall_one]))
    forward(arrive[0], tall_one)
    if zn > 2:
        forward(arrive[1], every)
    spread_y(0)
    for g in arrive[2:]:
        forward(g, every)
    for i, g in enumerate(pieces):
        spread_z(g)
        if i > 0:
            spread_y(pieces[i - 1])
    spread_y(pieces[-1])
    for c in own_copies[1:]:
        c.wait()
    for g in range(zn):
        for c in x_weights(g):
            c.wait_recv()

    unit_at = lax.broadcasted_iota(jnp.int32, (1, taken * LANES), 1)
    mine = unit_at >= jnp.where(z == 0, 0, (first_tile(z - 1) + taken - first_tile(z)) * LANES)

    def feed(g, buf):
        core_token_came(g).wait_recv()
        both_token_came(g).wait_recv()
        block = tokens[zx(g)]
        gate = mm(block, gbuf[...])
        up = mm(block, ubuf[...])
        hidden[...] = jnp.where(mine, gate / (1.0 + jnp.exp(-gate)) * up, 0.0).astype(bf16)

        def down(i, _):
            cols = pl.ds(pl.multiple_of(i * step, step), step)
            part[buf, :, cols] = mm(hidden[...], dbuf[:, cols])
            return _

        lax.fori_loop(0, width // step, down, 0)

    def z_copy(g):
        return remote(z_out.at[g], z_in.at[g], z_s.at[g], z_r.at[g], at(zx(g), x, tp))

    def send_z(g):
        y_copy(g).wait_recv()
        if is_own(g):
            kept[g] = kept[g] + y_in[g].astype(f32)
        else:
            z_out[g] = (kept[g] + y_in[g].astype(f32)).astype(bf16)
            z_copy(g).start()

    order = pieces[1:] + pieces[:1] + [own_group]
    for i, g in enumerate(order):
        feed(g, i % 2)
        send_core(g, i % 2)
        if i >= 1:
            send_y(order[i - 1], (i - 1) % 2)
        if i >= 2:
            send_z(order[i - 2])
    send_y(order[-1], (zn - 1) % 2)
    send_z(order[-2])
    send_z(order[-1])
    total = middle[...] + kept[0]
    for g in range(1, zn):
        z_copy(g).wait_recv()
        total = total + z_in[g].astype(f32)
    out[...] = total.astype(bf16)

    for g in range(1, zn):
        for c in z_weights(g):
            c.wait_send()
        z_copy(g).wait_send()
        zz = zx(g)
        moved_on = ((zz < z) & (z < zn - 1)) | ((zz > z) & (z > 0))
        when(moved_on, up_copy(zz, ring_s.at[g]).wait_send)
    for g in range(zn):
        for c in x_weights(g):
            c.wait_send()
        y_token(g).wait_send()
        core_token(g).wait_send()
        both_token(g).wait_send()
    for i in range(zn + 1):
        core_copy(i).wait_send()
        y_copy(i).wait_send()
    sum_copy.wait_send()
    when(z < zn - 1, state_copy.wait_send)
    when(z < zn - 1, up_copy(z, own_s.at[0]).wait_send)
    when(z > 0, down_copy(z, own_s.at[1]).wait_send)


def fits(mesh, *arrays):
    sp, tp = mesh.shape["sp"], mesh.shape["tp"]
    heads, positions = arrays[8].shape
    units = arrays[12].shape[1]
    zn = sp // PAIR
    return (
        tp == 4
        and sp % PAIR == 0
        and zn > 1
        and zn & (zn - 1) == 0
        and heads % 2 == 0
        and positions % LANES == 0
        and positions == tp * arrays[0].shape[0]
        and units % LANES == 0
        and units // LANES >= zn
        and arrays[12].shape[0] % LANES == 0
        and arrays[0].shape[1] % (4 * LANES) == 0
    )


def fused(
    residual, query, key, value, fading, step_size, switch, bias, surplus, head_gain, out_proj,
    row_gain, gate_up, expand, contract,
):
    zn = lax.axis_size("sp") // PAIR
    rows, width = residual.shape
    channels, positions = query.shape
    pairs, blocks = channels // LANES, positions // LANES
    many = pairs * blocks
    taken = -(-(gate_up.shape[1] // LANES) // zn) * LANES
    square = (LANES, LANES)
    half = (HEAD, LANES)
    vmem, dma = pltpu.VMEM, pltpu.SemaphoreType.DMA
    scratch = [
        vmem(out_proj.shape, bf16),
        vmem((width, taken), bf16),
        vmem((width, taken), bf16),
        vmem((taken, width), bf16),
        vmem((2 * many, *square), f32),
        vmem((2 * many, *square), f32),
        vmem((2 * many, *square), f32),
        vmem((many, *square), f32),
        vmem((many, *half), f32),
        vmem((many, *half), f32),
        vmem((many, *square), f32),
        vmem((many, *square), f32),
        vmem((pairs, *square), f32),
        vmem((pairs, *square), bf16),
        vmem((pairs, *square), bf16),
        vmem((pairs, *square), f32),
        vmem((pairs, *half), bf16),
        vmem((pairs, *half), bf16),
        vmem((pairs, *half), f32),
        vmem((positions, channels), bf16),
        vmem((2, positions, width), f32),
        vmem((zn + 1, rows, width), f32),
        vmem((zn + 1, 2, rows, width), bf16),
        vmem((zn + 1, 2, rows, width), bf16),
        vmem((zn + 1, rows, width), bf16),
        vmem((zn + 1, rows, width), bf16),
        vmem((zn, rows, width), bf16),
        vmem((zn, rows, width), bf16),
        vmem((rows, width), f32),
        vmem((zn, positions, width), bf16),
        vmem((positions, taken), bf16),
        dma((4,)),
        dma((zn, 3)), dma((zn, 3)), dma((zn, 3)), dma((zn, 3)),
        dma((2,)), dma((2,)),
        dma((zn + 1,)), dma((zn + 1,)), dma((zn + 1,)), dma((zn + 1,)), dma((zn,)), dma((zn,)),
        dma((2,)), dma((zn,)), dma((zn,)),
        dma((zn,)), dma((zn,)), dma((zn,)), dma((zn,)), dma((zn,)), dma((zn,)),
    ]
    inside = pl.BlockSpec(memory_space=pltpu.VMEM)
    outside = pl.BlockSpec(memory_space=pl.ANY)
    return pl.pallas_call(
        functools.partial(layer_kernel, zn),
        out_shape=jax.ShapeDtypeStruct((rows, width), bf16),
        in_specs=[inside] * 11 + [outside] * 4,
        out_specs=inside,
        scratch_shapes=scratch,
        compiler_params=pltpu.CompilerParams(
            collective_id=0, has_side_effects=True, vmem_limit_bytes=60 << 20
        ),
        name="layer",
    )(
        residual, query, key, value, fading, step_size, switch, bias.reshape(pairs, LANES), surplus,
        head_gain.reshape(pairs, LANES), row_gain[None, :], out_proj, gate_up, expand, contract,
    )


def solution(mesh):
    placed = (
        P(("sp", "tp"), None),
        P("tp", "sp"),
        P("tp", "sp"),
        P("tp", "sp"),
        P("tp", "sp"),
        P("tp", "sp"),
        P("tp", "sp"),
        P("tp"),
        P("tp", "sp"),
        P("tp"),
        P("tp", None),
        P(),
        P("sp", "tp"),
        P("sp", "tp"),
        P("tp", "sp"),
    )

    def layer(*arrays):
        return (fused if fits(mesh, *arrays) else local)(*arrays)


    return jax.shard_map(
        layer, mesh=mesh, in_specs=placed, out_specs=P(("sp", "tp"), None), check_vma=False
    )
```

```python
import functools
import jax
import jax.numpy as jnp
from jax import lax
from jax.experimental import pallas as pl
from jax.experimental.pallas import tpu as pltpu
from jax.sharding import PartitionSpec as P

HEAD = 64
BLOCK = 64


norm_eps = 1e-06
group_eps = 0.00064
key_eps = 1e-06
highest = lax.Precision.HIGHEST
high = lax.Precision.HIGH


def shifted(x, axis, by):
    n = lax.axis_size(axis)
    return lax.ppermute(x, axis, [(i, (i + by) % n) for i in range(n)])


def paired(x):
    n = lax.axis_size("sp")
    return lax.ppermute(x, "sp", [(i, i ^ 1) for i in range(n)])


def around(first, second):
    n = lax.axis_size("sp")
    ring = n // 2
    half = ring // 2

    def hop(x, by):
        return lax.ppermute(x, "sp", [(i, (i + 2 * by) % n) for i in range(n)])

    out = [[None] * ring, [None] * ring]
    for place, piece in enumerate((first, second)):
        out[place][0] = piece
        up = down = piece
        for step in range(1, half):
            up = hop(up, 1)
            down = hop(down, -1)
            out[place][ring - step] = up
            out[place][step] = down
        if ring > 1:
            out[place][half] = hop(up, 1) if place == 0 else hop(down, -1)
    return out


def rolled(x, by):
    return lax.dynamic_slice_in_dim(jnp.concatenate([x, x], axis=1), by, x.shape[1], 1)


def carried_in(summary):
    n = lax.axis_size("sp")
    carry_map, carry_add = summary
    both = jnp.concatenate([carry_map, carry_add], axis=1).astype(jnp.bfloat16)
    width = carry_map.shape[1]
    state = jnp.zeros_like(carry_add)
    for back in range(n - 1, 0, -1):
        came = lax.ppermute(both, "sp", [(i, i + back) for i in range(n - back)])
        came = came.astype(jnp.float32)
        state = (
            jnp.einsum("hvk,hkj->hvj", state, came[:, :width], precision=high)
            + came[:, width:]
        )
    return state


def by_blocks(source, attention_group_count, position_count):
    return (
        source.astype(jnp.float32)
        .reshape(attention_group_count, HEAD, position_count // BLOCK, BLOCK)
        .transpose(0, 2, 3, 1)
    )


def compose(earlier, latter):
    return (
        jnp.einsum("...ij,...jk->...ik", earlier[0], latter[0], precision=high),
        jnp.einsum("...ij,...jk->...ik", earlier[1], latter[0], precision=high) + latter[1],
    )


def unit_lower_solve(mutual, right_side):
    power = -mutual
    solved = right_side
    for level in range((BLOCK - 1).bit_length()):
        solved = solved + jnp.einsum("hbts,hbsn->hbtn", power, solved, precision=highest)
        if level + 1 < (BLOCK - 1).bit_length():
            power = jnp.einsum("hbts,hbsu->hbtu", power, power, precision=highest)
    return solved


def rms_rows(middle, dense_block_scaler):
    scale_rows = lax.rsqrt(jnp.mean(middle * middle, axis=-1, keepdims=True) + norm_eps)
    return (middle * scale_rows * dense_block_scaler).astype(jnp.bfloat16)


def local(
    residual_matrix,
    query_vectors,
    lookup_vectors,
    payload_vectors,
    fading_dependent_term,
    step_size_preactivation,
    attention_result_switch,
    fading_bias_vector,
    surplus_forgetting,
    per_group_scaler,
    attention_result_matrix,
    dense_block_scaler,
    switching_matrix,
    expanding_matrix,
    contracting_matrix,
):
    count_sp, count_tp = lax.axis_size("sp"), lax.axis_size("tp")
    parity = lax.axis_index("sp") % 2
    ring_place = lax.axis_index("sp") // 2
    units = switching_matrix.shape[1] // 2

    def part(x, which, axis):
        return lax.dynamic_slice_in_dim(x, which * units, units, axis)

    def gate_up(which):
        return jnp.concatenate(
            [part(switching_matrix, which, 1), part(expanding_matrix, which, 1)], axis=1
        )

    wide_pieces = around(gate_up(parity), paired(gate_up(1 - parity)))
    down_pieces = around(
        part(contracting_matrix, parity, 0), part(contracting_matrix, 1 - parity, 0)
    )
    attention_group_count = surplus_forgetting.shape[0]
    position_count = surplus_forgetting.shape[1]
    block_count = position_count // BLOCK
    read_rows = by_blocks(query_vectors, attention_group_count, position_count)
    key_rows = by_blocks(lookup_vectors, attention_group_count, position_count)
    value_rows = by_blocks(payload_vectors, attention_group_count, position_count)
    fading_preactivation = by_blocks(
        fading_dependent_term, attention_group_count, position_count
    ) + fading_bias_vector.reshape(attention_group_count, 1, 1, HEAD)
    log_fading_factor = -jnp.exp(
        -jax.nn.softplus(-fading_preactivation) - 0.5
    ) + surplus_forgetting.reshape(attention_group_count, block_count, BLOCK, 1)
    learn_rate = jax.nn.sigmoid(
        by_blocks(step_size_preactivation, attention_group_count, position_count)
    )
    unit_keys = key_rows * lax.rsqrt(jnp.sum(key_rows * key_rows, axis=-1, keepdims=True) + key_eps)
    scaled = key_rows * learn_rate
    removal = unit_keys * learn_rate
    cum_after = jnp.cumsum(log_fading_factor, axis=2)
    before = cum_after - log_fading_factor
    cum_final = cum_after[:, :, -1:, :]
    probe_keys = unit_keys * jnp.exp(before)
    removal_in = removal * jnp.exp(-cum_after)
    scaled_in = scaled * jnp.exp(-cum_after)
    reads_out = read_rows * jnp.exp(cum_after)
    position = jnp.arange(BLOCK)
    strict = position[:, None] > position[None, :]
    up_to = position[:, None] >= position[None, :]
    mutual = jnp.where(
        strict, jnp.einsum("hbtn,hbsn->hbts", probe_keys, removal_in, precision=high), 0.0
    )
    through = jnp.where(
        strict, jnp.einsum("hbtn,hbsn->hbts", probe_keys, scaled_in, precision=high), 0.0
    )
    right_side = jnp.concatenate(
        [probe_keys, jnp.einsum("hbts,hbsn->hbtn", through, value_rows, precision=high)], axis=-1
    )
    solved = unit_lower_solve(mutual, right_side)
    basis_part = solved[..., :HEAD]
    offset = solved[..., HEAD:]
    removal_end = removal * jnp.exp(cum_final - cum_after)
    scaled_end = scaled * jnp.exp(cum_final - cum_after)
    carry_map = jnp.eye(HEAD, dtype=jnp.float32) * jnp.exp(cum_final) - jnp.einsum(
        "hbtk,hbtj->hbkj", basis_part, removal_end, precision=high
    )
    carry_add = jnp.einsum(
        "hbtv,hbtj->hbvj", value_rows, scaled_end, precision=high
    ) - jnp.einsum("hbtv,hbtj->hbvj", offset, removal_end, precision=high)
    summary = (carry_map[:, 0], carry_add[:, 0])
    for block in range(1, block_count):
        summary = compose(summary, (carry_map[:, block], carry_add[:, block]))
    carried = carried_in(summary)
    starts = [carried]
    for block in range(block_count - 1):
        carried = (
            jnp.einsum("hvk,hkj->hvj", carried, carry_map[:, block], precision=high)
            + carry_add[:, block]
        )
        starts.append(carried)
    starts = jnp.stack(starts, axis=1)
    removed = -jnp.einsum("hbtk,hbvk->hbtv", basis_part, starts, precision=high) - offset
    reach_removal = jnp.where(
        up_to, jnp.einsum("hbtn,hbsn->hbts", reads_out, removal_in, precision=high), 0.0
    )
    reach_value = jnp.where(
        up_to, jnp.einsum("hbtn,hbsn->hbts", reads_out, scaled_in, precision=high), 0.0
    )
    outputs = (
        jnp.einsum("hbtk,hbvk->hbtv", reads_out, starts, precision=high)
        + jnp.einsum("hbts,hbsv->hbtv", reach_removal, removed, precision=high)
        + jnp.einsum("hbts,hbsv->hbtv", reach_value, value_rows, precision=high)
    )
    centred = outputs - jnp.mean(outputs, axis=-1, keepdims=True)
    normed_heads = centred * lax.rsqrt(
        jnp.mean(centred * centred, axis=-1, keepdims=True) + group_eps
    )
    normed_heads = normed_heads.transpose(0, 3, 1, 2).reshape(
        attention_group_count * HEAD, position_count
    )
    mixed_out = (
        normed_heads * per_group_scaler[:, None] * attention_result_switch.astype(jnp.float32)
    ).astype(jnp.bfloat16)
    tp_place = lax.axis_index("tp")
    rows = residual_matrix.shape[0]
    partial = jnp.einsum(
        "ct,cd->td", mixed_out, attention_result_matrix, preferred_element_type=jnp.float32
    )

    def rows_of(x, by):
        owner = (tp_place + by) % count_tp
        return lax.dynamic_slice_in_dim(x, owner * rows, rows, 0)

    sent = partial.astype(jnp.bfloat16)
    middle = residual_matrix.astype(jnp.float32) + rows_of(partial, 0)
    for by in range(1, count_tp):
        middle = middle + shifted(rows_of(sent, by), "tp", by).astype(jnp.float32)
    normed = rms_rows(middle, dense_block_scaler)
    depth = switching_matrix.shape[0]

    def column_blocks(x):
        return [x[:, i * depth : (i + 1) * depth] for i in range(x.shape[1] // depth)]

    turned = rolled(normed, ring_place * 2 * depth)
    blocks = column_blocks(turned)
    flipped = jnp.concatenate([blocks[i ^ 1] for i in range(count_sp)], axis=1)
    near = jnp.where(parity == 0, turned, flipped)
    far = paired(jnp.where(parity == 0, flipped, turned))

    def spread(x):
        return jnp.concatenate([x] + [shifted(x, "tp", by) for by in range(1, count_tp)], axis=0)

    def stacked(pieces):
        return jnp.concatenate([x for pair in zip(*pieces) for x in pair], axis=0)

    wide_weight = stacked(wide_pieces)

    def units_of(x):
        both = jnp.dot(x, wide_weight, preferred_element_type=jnp.float32)
        return (jax.nn.silu(both[:, :units]) * both[:, units:]).astype(jnp.bfloat16)

    near_units = units_of(spread(near))
    near_sent = paired(near_units)
    far_units = units_of(spread(far))
    far_sent = paired(far_units)
    down_own = jnp.concatenate(down_pieces[0], axis=1)
    down_other = jnp.concatenate(down_pieces[1], axis=1)

    def summed(own, other):
        product = (
            jnp.dot(own, down_own, preferred_element_type=jnp.float32)
            + jnp.dot(other, down_other, preferred_element_type=jnp.float32)
        ).astype(jnp.bfloat16)
        total = product[:rows].astype(jnp.float32)
        for by in range(1, count_tp):
            total = total + shifted(product[by * rows : (by + 1) * rows], "tp", -by).astype(
                jnp.float32
            )
        return total

    far_sum = paired(summed(far_units, near_sent).astype(jnp.bfloat16)).astype(jnp.float32)
    near_sum = summed(near_units, far_sent)
    even = column_blocks(jnp.where(parity == 0, near_sum, far_sum))
    odd = column_blocks(jnp.where(parity == 0, far_sum, near_sum))
    columns = jnp.concatenate([x for pair in zip(even, odd) for x in pair], axis=1)
    channel_out = rolled(columns, (count_sp // 2 - ring_place) % (count_sp // 2) * 2 * depth)
    return (middle + channel_out).astype(jnp.bfloat16)


LANES = 128
PAIR = 2
CUTS = 4
MESH = pl.DeviceIdType.MESH
f32, bf16 = jnp.float32, jnp.bfloat16
NN = (((1,), (0,)), ((), ()))
NT = (((1,), (1,)), ((), ()))


def mm(a, b, dims=NN):
    return lax.dot_general(a, b, dims, preferred_element_type=f32)


def split(x):
    top = x.astype(bf16)
    return top, (x - top.astype(f32)).astype(bf16)


def mm3(a, b, dims=NN):
    (ah, al), (bh, bl) = split(a), split(b)
    axis = dims[0][1][0]
    return mm(
        jnp.concatenate([ah, al], axis=1), jnp.concatenate([bh, bh], axis=axis), dims
    ) + mm(ah, bl, dims)


def mm2(a, b, dims=NN):
    axis = dims[0][1][0]
    return mm(
        jnp.concatenate([a, a], axis=1), jnp.concatenate(split(b), axis=axis), dims
    )


def grid_of(rows):
    return (
        lax.broadcasted_iota(jnp.int32, (rows, LANES), 0),
        lax.broadcasted_iota(jnp.int32, (rows, LANES), 1),
    )


def heads_apart(x):
    row, col = grid_of(LANES)
    return jnp.where((row < HEAD) == (col < HEAD), jnp.concatenate([x, x], axis=0), 0.0)


def inverses(mutuals):
    row, col = grid_of(LANES)
    eye = jnp.where(row == col, 1.0, 0.0)
    solved = [eye - jnp.where((row % 2 == 0) & (col == row + 1), a, 0.0) for a in mutuals]
    for level in range(1, LANES.bit_length() - 1):
        size = 1 << level
        cross = ((row // size) % 2 == 0) & (col // size == row // size + 1)
        rounded = [s.astype(bf16) for s in solved]
        moved = [
            mm(r, jnp.where(cross, a, 0.0).astype(bf16)).astype(bf16)
            for r, a in zip(rounded, mutuals)
        ]
        solved = [s - mm(m, r) for s, m, r in zip(solved, moved, rounded)]
    rest = [eye - s - mm3(a, s) for a, s in zip(mutuals, solved)]
    return [s + mm(s.astype(bf16), r.astype(bf16)) for s, r in zip(solved, rest)]


def layer_kernel(
    zn,
    resid, query, key, value, fading, step_size, switch, bias, surplus, head_gain, row_gain,
    wo, wg, wu, wd,
    out,
    wo_v, gbuf, ubuf, dbuf,
    solved_s, reach_r, reach_v, reads_s, map_s, add_s, read_map, read_add,
    own_sum, sum_out, sum_in, pair_sum, state_out, state_in, entering,
    mixed, part, kept, core_out, core_in, y_out, y_in, z_out, z_in,
    middle, tokens, hidden,
    pair_out, pair_in, step_in,
    local_sem, pair_sem, step_r, wz_s, wz_r, wx_s, wx_r, sum_sem, state_sem,
    core_s, core_r, y_s, y_r, z_s, z_r,
    own_s, ring_s, ring_r, ty_s, ty_r, tc_s, tc_r, td_s, td_r,
):
    sp, tp = lax.axis_index("sp"), lax.axis_index("tp")
    z, x = sp // PAIR, sp % PAIR
    t_core = tp + 1 - 2 * (tp % 2)
    t_y = (tp + 2) % 4
    t_both = (t_core + 2) % 4
    rows, width = resid.shape
    positions = query.shape[1]
    blocks = positions // LANES
    pairs = query.shape[0] // LANES
    depth = wg.shape[0]
    tiles = wg.shape[1] // LANES
    base, spare = tiles // zn, tiles % zn
    bits = (zn - 1).bit_length()

    own_group = 0

    def is_own(g):
        return isinstance(g, int) and g == own_group

    def zx(g):
        return sum(((z // (1 << i) + g // (1 << i)) % 2) * (1 << i) for i in range(bits))

    def at(zz, xx, tt):
        return {"sp": zz * PAIR + xx, "tp": tt}

    def first_tile(zz):
        return zz * base + sum((zz + zn - 1 - i) // zn for i in range(spare))

    def longer(zz):
        return zz < spare

    def remote(src, dst, send, recv, to):
        return pltpu.make_async_remote_copy(
            src_ref=src, dst_ref=dst, send_sem=send, recv_sem=recv, device_id=to, device_id_type=MESH
        )

    x_peer, y_peer, core_peer = at(z, 1 - x, tp), at(z, x, t_y), at(z, x, t_core)

    barrier = pltpu.get_barrier_semaphore()
    peers = [x_peer, y_peer, core_peer] + [at(zx(g), x, tp) for g in range(1, zn)]
    for peer in peers:
        pl.semaphore_signal(barrier, inc=1, device_id=peer, device_id_type=MESH)
    pl.semaphore_wait(barrier, len(peers))

    runs = [(0, base)] + ([(base, 1)] if spare else [])

    def run_start(zz, run):
        short = (zz + zn - spare) // zn if run[0] else 0
        return pl.multiple_of((first_tile(zz) + run[0] - short) * LANES, LANES)

    def wide(ref, zz, run):
        first = run_start(zz, run)
        return ref.at[:, pl.ds(first, run[1] * LANES)]

    def tall(ref, zz, run):
        first = run_start(zz, run)
        return ref.at[pl.ds(first, run[1] * LANES), :]

    def slots(place):
        span = pl.ds(pl.multiple_of(place * depth, depth), depth)
        units = [slice(a * LANES, (a + n) * LANES) for a, n in runs]
        return (
            [w.at[span, u] for u in units for w in (gbuf, ubuf)]
            + [dbuf.at[u, span] for u in units]
        )

    def cut(zz):
        return [wide(w, zz, run) for run in runs for w in (wg, wu)] + [
            tall(wd, zz, run) for run in runs
        ]

    is_spare = [False, False, True, True, False, True] if spare else [False] * 3
    count = len(is_spare)
    every, wide_two, tall_one = range(count), range(count * 2 // 3), range(count * 2 // 3, count)

    def each(copies, which, zz, action):
        for i in which:
            if is_spare[i]:
                pl.when(longer(zz))(functools.partial(action, copies[i]))
            else:
                action(copies[i])

    def begin(copies, which, zz):
        each(copies, which, zz, lambda c: c.start())

    wo_copy = pltpu.make_async_copy(wo, wo_v, local_sem.at[count])
    own_copies = [
        pltpu.make_async_copy(a, b, local_sem.at[i])
        for i, (a, b) in enumerate(zip(cut(z), slots(sp)))
    ]

    def z_weights(g):
        return [
            remote(a, b, wz_s.at[g, i], wz_r.at[g, i], at(zx(g), x, tp))
            for i, (a, b) in enumerate(zip(cut(zx(g)), slots(sp)))
        ]

    def x_weights(g):
        there = slots(zx(g) * PAIR + x)
        return [
            remote(a, b, wx_s.at[g, i], wx_r.at[g, i], x_peer)
            for i, (a, b) in enumerate(zip(cut(z) if is_own(g) else there, there))
        ]

    def column(ref, hp):
        return jnp.broadcast_to(ref[pl.ds(hp, 1), :], (LANES, LANES)).T

    def column(ref, hp):
        return jnp.broadcast_to(ref[pl.ds(hp, 1), :], (LANES, LANES)).T

    def start_up(g, which):
        pl.when(zx(g) > z)(lambda: begin(z_weights(g), which, zx(g)))

    def start_down(g, which):
        pl.when(zx(g) < z)(lambda: begin(z_weights(g), which, zx(g)))

    def forward(g, which):
        onward = dict(zip(every, x_weights(g)))
        came = z_weights(g)

        def move(i):
            came[i].wait_recv()
            onward[i].start()

        each(list(every), which, z, move)

    inner = ((z + 1) // 2) % 2
    rest = list(range(4, zn))
    arrive = [3 - inner, 1, 2 + inner] + rest if zn >= 4 else [1]
    pieces = [1, 2 + inner, 3 - inner] + rest if zn >= 4 else [1]

    far_first = list(range(zn - 1, 0, -1))
    wo_copy.start()
    begin(own_copies, every, z)
    begin(x_weights(0), every, z)
    if zn >= 4:

        @pl.when(inner == 1)
        def _():
            for g in [2, 3, 1] + rest:
                start_down(g, every)

        @pl.when(inner == 0)
        def _():
            for g in far_first:
                start_down(g, every)

    else:
        start_down(1, every)

    @pl.when(z == 0)
    def _():
        for g in far_first[:-1]:
            begin(z_weights(g), every, zx(g))

    if spare:

        @pl.when(z >= spare)
        def _():
            gbuf[:, base * LANES :] = jnp.zeros((width, LANES), bf16)
            ubuf[:, base * LANES :] = jnp.zeros((width, LANES), bf16)
            dbuf[base * LANES :, :] = jnp.zeros((LANES, width), bf16)

    row, col = grid_of(LANES)
    strict, up_to = row < col, row <= col
    row_h, col_h = grid_of(HEAD)
    left = col_h < HEAD

    def prepared(hp, mutuals, grams):
        r0 = pl.multiple_of(hp * LANES, LANES)
        here = pl.ds(r0, LANES)
        keys = key[here, :].astype(f32)
        extra = jnp.concatenate(
            [
                jnp.broadcast_to(surplus[pl.ds(2 * hp + i, 1), :], (HEAD, positions))
                for i in range(2)
            ],
            axis=0,
        )
        pre = fading[here, :].astype(f32) + jnp.tile(column(bias, hp), (1, blocks))
        log_fade = -0.6065306597126334 / (1.0 + jnp.exp(-pre)) + extra
        rate = 1.0 / (1.0 + jnp.exp(-step_size[here, :].astype(f32)))
        unit = jnp.concatenate(
            [
                h * lax.rsqrt(jnp.sum(h * h, axis=0, keepdims=True) + key_eps)
                for h in (keys[:HEAD], keys[HEAD:])
            ],
            axis=0,
        )
        removal, scaled = unit * rate, keys * rate
        reads = query[here, :].astype(f32)
        ones = jnp.where(up_to, 1.0, 0.0).astype(bf16)
        ends, probes = [], []
        for b in range(blocks):
            lanes = slice(b * LANES, (b + 1) * LANES)
            fade = log_fade[:, lanes]
            f1 = fade.astype(bf16)
            left_over = fade - f1.astype(f32)
            f2 = left_over.astype(bf16)
            f3 = (left_over - f2.astype(f32)).astype(bf16)
            after = mm(f1, ones) + (mm(f2, ones) + mm(f3, ones))
            before = after - fade
            mid, last = after[:, HEAD - 1 : HEAD], after[:, LANES - 1 :]
            shrink = jnp.exp(mid - after)
            probe = unit[:, lanes] * jnp.exp(before - mid)
            read = reads[:, lanes] * jnp.exp(after - mid)
            removal_in, scaled_in = removal[:, lanes] * shrink, scaled[:, lanes] * shrink
            to_mid, to_end = jnp.exp(mid), jnp.exp(last - mid)
            reads_s[hp * blocks + b] = read * to_mid
            probes.append(probe * to_mid)
            ends.append((removal_in * to_end, scaled_in * to_end, jnp.exp(last)))
            both_in = [split(removal_in), split(scaled_in)]
            top, low = split(jnp.concatenate([probe, read], axis=1))
            for hh in range(2):
                own = slice(hh * HEAD, (hh + 1) * HEAD)
                turned = jnp.concatenate(
                    [
                        jnp.concatenate([h[own], l[own]], axis=0).astype(f32).T.astype(bf16)
                        for h, l in both_in
                    ],
                    axis=0,
                )
                right = jnp.concatenate(
                    [top[own], top[own], low[own], jnp.zeros_like(low[own])], axis=0
                )
                gram = mm(jnp.concatenate([turned, turned], axis=1), right)
                mutuals.append(jnp.where(strict, gram[:LANES, :LANES], 0.0))
                place = (hp * blocks + b) * 2 + hh
                reach_r[place] = jnp.where(up_to, gram[:LANES, LANES:], 0.0)
                reach_v[place] = jnp.where(up_to, gram[LANES:, LANES:], 0.0)
                grams.append(jnp.where(strict, gram[LANES:, :LANES], 0.0))
        return ends, probes

    def summed(hp, ends, probes, inverse, grams):
        values = value[pl.ds(pl.multiple_of(hp * LANES, LANES), LANES), :]
        total = None
        for b in range(blocks):
            lanes = slice(b * LANES, (b + 1) * LANES)
            removal_end, scaled_end, fade_end = ends[b]
            taken_out, added = [], []
            for hh in range(2):
                own = slice(hh * HEAD, (hh + 1) * HEAD)
                vals = values[own, lanes]
                right = jnp.concatenate([probes[b][own], mm2(vals, grams[b * 2 + hh])], axis=0)
                solved = mm3(right, inverse[b * 2 + hh])
                solved_s[(hp * blocks + b) * 2 + hh] = solved
                taken_out.append(mm3(solved, removal_end, NT))
                added.append(mm2(vals, scaled_end, NT))
            both = [
                jnp.where(left, taken_out[0][i], taken_out[1][i])
                for i in (slice(0, HEAD), slice(HEAD, LANES))
            ]
            fade_both = jnp.where(left, fade_end[:HEAD], fade_end[HEAD:])
            carry_map = jnp.where(row_h == col_h % HEAD, fade_both, 0.0) - both[0]
            carry_add = jnp.where(left, added[0], added[1]) - both[1]
            map_s[hp * blocks + b] = carry_map
            add_s[hp * blocks + b] = carry_add
            if total is None:
                total = jnp.concatenate([carry_map, carry_add], axis=0)
            else:
                total = mm3(total, heads_apart(carry_map)) + jnp.concatenate(
                    [jnp.zeros_like(carry_add), carry_add], axis=0
                )
        own_sum[hp] = total
        sum_out[hp] = total.astype(bf16)

    together = 2 if pairs % 2 == 0 else 1

    def sum_copy(i):
        share = pl.ds(i * together, together)
        return remote(sum_out.at[share], sum_in.at[share], sum_sem.at[0, i], sum_sem.at[1, i], x_peer)

    def first_part(i, _):
        mutuals, grams, ready = [], [], []
        for j in range(together):
            ready.append(prepared(i * together + j, mutuals, grams))
        inverse = inverses(mutuals)
        for j in range(together):
            span = slice(j * 2 * blocks, (j + 1) * 2 * blocks)
            summed(i * together + j, *ready[j], inverse[span], grams[span])
        sum_copy(i).start()
        return _

    lax.fori_loop(0, pairs // together, first_part, 0)


    def reading_part(hp, _):
        here = pl.ds(pl.multiple_of(hp * LANES, LANES), LANES)
        for b in range(blocks):
            lanes = slice(b * LANES, (b + 1) * LANES)
            maps, adds = [], []
            reads = reads_s[hp * blocks + b]
            values = value[here, lanes]
            for hh in range(2):
                own = slice(hh * HEAD, (hh + 1) * HEAD)
                place = (hp * blocks + b) * 2 + hh
                gone = mm3(solved_s[place], reach_r[place])
                maps.append(reads[own] - gone[:HEAD])
                adds.append(mm2(values[own], reach_v[place]) - gone[HEAD:])
            read_map[hp * blocks + b] = jnp.concatenate(maps, axis=0)
            read_add[hp * blocks + b] = jnp.concatenate(adds, axis=0)
        return _

    lax.fori_loop(0, pairs, reading_part, 0)
    for i in range(pairs // together):
        sum_copy(i).wait_recv()

    def pair_part(hp, _):
        got, own = sum_in[hp].astype(f32), own_sum[hp]
        first = jnp.where(x == 0, own, got)
        second = jnp.where(x == 0, got, own)
        pair_sum[hp] = mm3(first, heads_apart(second[:HEAD])) + jnp.concatenate(
            [jnp.zeros((HEAD, LANES), f32), second[HEAD:]], axis=0
        )
        return _

    lax.fori_loop(0, pairs, pair_part, 0)
    if zn >= 4:

        @pl.when(inner == 0)
        def _():
            forward(arrive[0], every)


    up_z, down_z = (z + 1) % zn, (z + zn - 1) % zn
    state_copy = remote(state_out, state_in, state_sem.at[0], state_sem.at[1], at(up_z, x, tp))

    @pl.when(z == 0)
    def _():
        state_in[...] = jnp.zeros_like(state_in)

    @pl.when(z > 0)
    def _():
        state_copy.wait_recv()

    def chain_part(hp, _):
        state_out[hp] = (
            mm2(state_in[hp], heads_apart(pair_sum[hp, :HEAD])) + pair_sum[hp, HEAD:]
        ).astype(bf16)
        return _

    lax.fori_loop(0, pairs, chain_part, 0)

    @pl.when(z < zn - 1)
    def _():
        state_copy.start()

    @pl.when(z == 0)
    def _():
        begin(z_weights(1), wide_two, zx(1))

    @pl.when(z > 0)
    def _():
        start_up(1, every)
        if zn >= 4:
            start_up(3, wide_two)
            start_up(2, every)
            start_up(3, tall_one)
            for g in rest:
                start_up(g, every)

    if zn >= 4:

        @pl.when(inner == 1)
        def _():
            forward(arrive[0], every)

    else:
        forward(arrive[0], every)


    def second_part(hp, _):
        r0 = pl.multiple_of(hp * LANES, LANES)
        here = pl.ds(r0, LANES)
        came = state_in[hp].astype(f32)
        gain = column(head_gain, hp)
        got = sum_in[hp].astype(f32)
        state = jnp.where(x == 0, came, mm3(came, heads_apart(got[:HEAD])) + got[HEAD:])
        for b in range(blocks):
            place = hp * blocks + b
            result = mm3(heads_apart(state), read_map[place]) + read_add[place]
            normed = []
            for h in (result[:HEAD], result[HEAD:]):
                centred = h - jnp.mean(h, axis=0, keepdims=True)
                normed.append(
                    centred * lax.rsqrt(jnp.mean(centred * centred, axis=0, keepdims=True) + group_eps)
                )
            lanes = slice(b * LANES, (b + 1) * LANES)
            done = jnp.concatenate(normed, axis=0) * gain * switch[here, lanes].astype(f32)
            mixed[lanes, here] = done.T.astype(bf16)
            if b + 1 < blocks:
                state = mm3(state, heads_apart(map_s[place])) + add_s[place]
        return _

    lax.fori_loop(0, pairs, second_part, 0)

    step = 4 * LANES
    wo_copy.wait()

    def project(i, _):
        cols = pl.ds(pl.multiple_of(i * step, step), step)
        part[0, :, cols] = mm(mixed[...], wo_v[:, cols])
        return _

    lax.fori_loop(0, width // step, project, 0)

    def rows_for(t):
        return pl.ds(pl.multiple_of(t * rows, rows), rows)

    def core_copy(i):
        return remote(core_out.at[i], core_in.at[i], core_s.at[i], core_r.at[i], core_peer)

    cuts = [slice(i * width // CUTS, (i + 1) * width // CUTS) for i in range(CUTS)]

    def y_copy(i, h):
        return remote(
            y_out.at[i, :, cuts[h]], y_in.at[i, :, cuts[h]], y_s.at[i, h], y_r.at[i, h], y_peer
        )

    def send_core(i, buf):
        core_out[i, 0] = part[buf, rows_for(t_core), :].astype(bf16)
        core_out[i, 1] = part[buf, rows_for(t_both), :].astype(bf16)
        core_copy(i).start()

    def send_y(i, buf):
        core_copy(i).wait_recv()
        if is_own(i):
            pair_copy.wait_recv()
        for h, cols in enumerate(cuts):
            across = part[buf, rows_for(t_y), cols] + core_in[i, 1, :, cols].astype(f32)
            along = part[buf, rows_for(tp), cols] + core_in[i, 0, :, cols].astype(f32)
            if beside(i):
                pair_out[0, :, cols] = along.astype(bf16)
                pair_out[1, :, cols] = across.astype(bf16)
                continue
            if is_own(i):
                across = across + pair_in[1, :, cols].astype(f32)
                along = along + pair_in[0, :, cols].astype(f32)
            y_out[i, :, cols] = across.astype(bf16)
            y_copy(i, h).start()
            kept[i, :, cols] = along
        if beside(i):
            pair_copy.start()

    def beside(g):
        return isinstance(g, int) and g == 1

    pair_copy = remote(pair_out, pair_in, pair_sem.at[2], pair_sem.at[3], at(zx(1), x, tp))
    send_core(zn, 0)
    send_y(zn, 0)
    for h in range(CUTS):
        y_copy(zn, h).wait_recv()
    middle[...] = resid[...].astype(f32) + (kept[zn] + y_in[zn].astype(f32))
    mid_rows = middle[...]
    scale = lax.rsqrt(jnp.mean(mid_rows * mid_rows, axis=-1, keepdims=True) + norm_eps)
    tokens[z, rows_for(tp), :] = (mid_rows * scale * row_gain[...]).astype(bf16)

    def piece(zz, t):
        return tokens.at[zz, rows_for(t), :]

    def up_copy(zz, sem):
        return remote(piece(zz, tp), piece(zz, tp), sem, ring_r.at[zz], at(up_z, x, tp))

    def down_copy(zz, sem):
        return remote(piece(zz, tp), piece(zz, tp), sem, ring_r.at[zz], at(down_z, x, tp))

    def when(cond, action):
        pl.when(cond)(action)

    def y_token(g):
        return remote(piece(zx(g), tp), piece(zx(g), tp), ty_s.at[g], ty_r.at[g], y_peer)

    def y_token_came(g):
        return remote(piece(zx(g), t_y), piece(zx(g), t_y), ty_s.at[g], ty_r.at[g], y_peer)

    def core_token(g):
        return remote(piece(zx(g), tp), piece(zx(g), tp), tc_s.at[g], tc_r.at[g], core_peer)

    def core_token_came(g):
        return remote(piece(zx(g), t_core), piece(zx(g), t_core), tc_s.at[g], tc_r.at[g], core_peer)

    def both_token(g):
        return remote(piece(zx(g), t_y), piece(zx(g), t_y), td_s.at[g], td_r.at[g], core_peer)

    def both_token_came(g):
        return remote(piece(zx(g), t_both), piece(zx(g), t_both), td_s.at[g], td_r.at[g], core_peer)

    def pair_token(zz):
        return remote(piece(zz, t_y), piece(zz, t_y), pair_sem.at[0], pair_sem.at[1], at(zx(1), x, tp))

    def spread_z(g):
        zz = zx(g)
        if is_own(g):
            when(z < zn - 1, lambda: up_copy(zz, own_s.at[0]).start())
            when(z > 0, lambda: down_copy(zz, own_s.at[1]).start())
        else:
            up_copy(zz, ring_s.at[g]).wait_recv()
            when((zz < z) & (z < zn - 1), lambda: up_copy(zz, ring_s.at[g]).start())
            when((zz > z) & (z > 0), lambda: down_copy(zz, ring_s.at[g]).start())
        if not beside(g):
            y_token(g).start()
        core_token(g).start()

    def spread_y(g):
        if beside(g):
            pair_token(zx(1)).wait_recv()
        else:
            y_token_came(g).wait_recv()
        both_token(g).start()
        if is_own(g):
            pair_token(z).start()

    spread_z(own_group)
    pl.when(z == 0)(lambda: begin(z_weights(1), tall_one, zx(1)))
    if zn > 2:
        forward(arrive[1], every)
    spread_y(0)
    for g in arrive[2:]:
        forward(g, every)
    near, far = pieces[0], pieces[1:]
    spread_z(near)
    if far:
        spread_z(far[0])

    @pl.when(inner == 1)
    def _():
        for g in far[1:]:
            spread_z(g)
        for g in pieces:
            spread_y(g)

    @pl.when(inner == 0)
    def _():
        spread_y(near)

    each(own_copies, every, z, lambda c: c.wait())
    for g in range(zn):
        each(x_weights(g), every, z, lambda c: c.wait_recv())

    def feed(g, buf):
        core_token_came(g).wait_recv()
        both_token_came(g).wait_recv()
        block = tokens[zx(g)]
        gate = mm(block, gbuf[...])
        up = mm(block, ubuf[...])
        hidden[...] = (gate / (1.0 + jnp.exp(-gate)) * up).astype(bf16)

        def down(i, _):
            cols = pl.ds(pl.multiple_of(i * step, step), step)
            part[buf, :, cols] = mm(hidden[...], dbuf[:, cols])
            return _

        lax.fori_loop(0, width // step, down, 0)

    def z_copy(g, h):
        return remote(
            z_out.at[g, :, cuts[h]], z_in.at[g, :, cuts[h]], z_s.at[g, h], z_r.at[g, h],
            at(zx(g), x, tp),
        )

    def step_copy(k, g, h):
        return remote(
            z_out.at[g, :, cuts[h]], step_in.at[k, :, cuts[h]], z_s.at[g, h], step_r.at[k, h],
            at(zx(1), x, tp),
        )

    def send_z(k, g):
        for h, cols in enumerate(cuts):
            y_copy(g, h).wait_recv()
            mine = kept[g, :, cols] + y_in[g, :, cols].astype(f32)
            if is_own(g):
                kept[g, :, cols] = mine
                continue

            @pl.when(inner == 0)
            def _():
                z_out[g, :, cols] = mine.astype(bf16)
                step_copy(k, g, h).start()

            @pl.when(inner == 1)
            def _():
                step_copy(k, g, h).wait_recv()
                z_out[g, :, cols] = (mine + step_in[k, :, cols].astype(f32)).astype(bf16)
                z_copy(g, h).start()

    feed(near, 2)
    send_core(near, 2)

    @pl.when(inner == 0)
    def _():
        for g in far[1:]:
            spread_z(g)
        send_y(near, 2)
        for g in far[:1]:
            spread_y(g)

    buf = 0
    for i, g in enumerate(far):
        buf = 1 - buf
        feed(g, buf)
        send_core(g, buf)
        if i == 0:
            pl.when(inner == 1)(lambda: send_y(near, 2))
        if i + 1 < len(far):
            send_y(g, buf)

            @pl.when(inner == 0)
            def _():
                spread_y(far[i + 1])

    if not far:
        pl.when(inner == 1)(lambda: send_y(near, 2))
    feed(own_group, 2)
    for g in far[-1:]:
        send_y(g, buf)
    send_core(own_group, 2)
    pl.when(inner == 1)(lambda: send_y(own_group, 2))
    for k, g in enumerate(far):
        if k + 1 == len(far):
            pl.when(inner == 0)(lambda: send_y(own_group, 2))
        send_z(k, g)
    send_z(0, own_group)
    for h, cols in enumerate(cuts):
        z_copy(far[0], h).wait_recv()
        total = middle[:, cols] + kept[0, :, cols] + z_in[far[0], :, cols].astype(f32)
        out[:, cols] = total.astype(bf16)

    for g in range(1, zn):
        each(z_weights(g), every, zx(g), lambda c: c.wait_send())
        for h in range(CUTS):
            if not beside(g):
                z_copy(g, h).wait_send()
        zz = zx(g)
        moved_on = ((zz < z) & (z < zn - 1)) | ((zz > z) & (z > 0))
        when(moved_on, up_copy(zz, ring_s.at[g]).wait_send)
    for g in range(zn):
        each(x_weights(g), every, z, lambda c: c.wait_send())
        if not beside(g):
            y_token(g).wait_send()
        core_token(g).wait_send()
        both_token(g).wait_send()
    for i in range(zn + 1):
        core_copy(i).wait_send()
        for h in range(CUTS):
            if not beside(i):
                y_copy(i, h).wait_send()
    for i in range(pairs // together):
        sum_copy(i).wait_send()
    pair_token(z).wait_send()
    pair_copy.wait_send()
    when(z < zn - 1, state_copy.wait_send)
    when(z < zn - 1, up_copy(z, own_s.at[0]).wait_send)
    when(z > 0, down_copy(z, own_s.at[1]).wait_send)


def fits(mesh, *arrays):
    sp, tp = mesh.shape["sp"], mesh.shape["tp"]
    heads, positions = arrays[8].shape
    units = arrays[12].shape[1]
    zn = sp // PAIR
    return (
        tp == 4
        and sp % PAIR == 0
        and zn == 4
        and heads % 2 == 0
        and positions % LANES == 0
        and positions == tp * arrays[0].shape[0]
        and units % LANES == 0
        and units // LANES >= zn
        and arrays[12].shape[0] % LANES == 0
        and arrays[0].shape[1] % (4 * LANES) == 0
    )


def fused(
    residual, query, key, value, fading, step_size, switch, bias, surplus, head_gain, out_proj,
    row_gain, gate_up, expand, contract,
):
    zn = lax.axis_size("sp") // PAIR
    rows, width = residual.shape
    channels, positions = query.shape
    pairs, blocks = channels // LANES, positions // LANES
    many = pairs * blocks
    taken = -(-(gate_up.shape[1] // LANES) // zn) * LANES
    square = (LANES, LANES)
    half = (HEAD, LANES)
    vmem, dma = pltpu.VMEM, pltpu.SemaphoreType.DMA
    scratch = [
        vmem(out_proj.shape, bf16),
        vmem((width, taken), bf16),
        vmem((width, taken), bf16),
        vmem((taken, width), bf16),
        vmem((2 * many, *square), f32),
        vmem((2 * many, *square), f32),
        vmem((2 * many, *square), f32),
        vmem((many, *square), f32),
        vmem((many, *half), f32),
        vmem((many, *half), f32),
        vmem((many, *square), f32),
        vmem((many, *square), f32),
        vmem((pairs, *square), f32),
        vmem((pairs, *square), bf16),
        vmem((pairs, *square), bf16),
        vmem((pairs, *square), f32),
        vmem((pairs, *half), bf16),
        vmem((pairs, *half), bf16),
        vmem((pairs, *half), f32),
        vmem((positions, channels), bf16),
        vmem((3, positions, width), f32),
        vmem((zn + 1, rows, width), f32),
        vmem((zn + 1, 2, rows, width), bf16),
        vmem((zn + 1, 2, rows, width), bf16),
        vmem((zn + 1, rows, width), bf16),
        vmem((zn + 1, rows, width), bf16),
        vmem((zn, rows, width), bf16),
        vmem((zn, rows, width), bf16),
        vmem((rows, width), f32),
        vmem((zn, positions, width), bf16),
        vmem((positions, taken), bf16),
        vmem((2, rows, width), bf16),
        vmem((2, rows, width), bf16),
        vmem((2, rows, width), bf16),
        dma((7,)), dma((4,)), dma((2, CUTS)),
        dma((zn, 6)), dma((zn, 6)), dma((zn, 6)), dma((zn, 6)),
        dma((2, pairs)), dma((2,)),
        dma((zn + 1,)), dma((zn + 1,)), dma((zn + 1, CUTS)), dma((zn + 1, CUTS)), dma((zn, CUTS)), dma((zn, CUTS)),
        dma((2,)), dma((zn,)), dma((zn,)),
        dma((zn,)), dma((zn,)), dma((zn,)), dma((zn,)), dma((zn,)), dma((zn,)),
    ]
    inside = pl.BlockSpec(memory_space=pltpu.VMEM)
    outside = pl.BlockSpec(memory_space=pl.ANY)
    return pl.pallas_call(
        functools.partial(layer_kernel, zn),
        out_shape=jax.ShapeDtypeStruct((rows, width), bf16),
        in_specs=[inside] * 11 + [outside] * 4,
        out_specs=inside,
        scratch_shapes=scratch,
        compiler_params=pltpu.CompilerParams(
            collective_id=0, has_side_effects=True, vmem_limit_bytes=60 << 20
        ),
        name="layer",
    )(
        residual, query, key, value, fading, step_size, switch, bias.reshape(pairs, LANES), surplus,
        head_gain.reshape(pairs, LANES), row_gain[None, :], out_proj, gate_up, expand, contract,
    )


def solution(mesh):
    placed = (
        P(("sp", "tp"), None),
        P("tp", "sp"),
        P("tp", "sp"),
        P("tp", "sp"),
        P("tp", "sp"),
        P("tp", "sp"),
        P("tp", "sp"),
        P("tp"),
        P("tp", "sp"),
        P("tp"),
        P("tp", None),
        P(),
        P("sp", "tp"),
        P("sp", "tp"),
        P("tp", "sp"),
    )

    def layer(*arrays):
        return (fused if fits(mesh, *arrays) else local)(*arrays)


    return jax.shard_map(
        layer, mesh=mesh, in_specs=placed, out_specs=P(("sp", "tp"), None), check_vma=False
    )
```

```python
import functools
import jax
import jax.numpy as jnp
from jax import lax
from jax.experimental import pallas as pl
from jax.experimental.pallas import tpu as pltpu
from jax.sharding import PartitionSpec as P

HEAD = 64
BLOCK = 64


norm_eps = 1e-06
group_eps = 0.00064
key_eps = 1e-06
highest = lax.Precision.HIGHEST
high = lax.Precision.HIGH


def shifted(x, axis, by):
    n = lax.axis_size(axis)
    return lax.ppermute(x, axis, [(i, (i + by) % n) for i in range(n)])


def paired(x):
    n = lax.axis_size("sp")
    return lax.ppermute(x, "sp", [(i, i ^ 1) for i in range(n)])


def around(first, second):
    n = lax.axis_size("sp")
    ring = n // 2
    half = ring // 2

    def hop(x, by):
        return lax.ppermute(x, "sp", [(i, (i + 2 * by) % n) for i in range(n)])

    out = [[None] * ring, [None] * ring]
    for place, piece in enumerate((first, second)):
        out[place][0] = piece
        up = down = piece
        for step in range(1, half):
            up = hop(up, 1)
            down = hop(down, -1)
            out[place][ring - step] = up
            out[place][step] = down
        if ring > 1:
            out[place][half] = hop(up, 1) if place == 0 else hop(down, -1)
    return out


def rolled(x, by):
    return lax.dynamic_slice_in_dim(jnp.concatenate([x, x], axis=1), by, x.shape[1], 1)


def carried_in(summary):
    n = lax.axis_size("sp")
    carry_map, carry_add = summary
    both = jnp.concatenate([carry_map, carry_add], axis=1).astype(jnp.bfloat16)
    width = carry_map.shape[1]
    state = jnp.zeros_like(carry_add)
    for back in range(n - 1, 0, -1):
        came = lax.ppermute(both, "sp", [(i, i + back) for i in range(n - back)])
        came = came.astype(jnp.float32)
        state = (
            jnp.einsum("hvk,hkj->hvj", state, came[:, :width], precision=high)
            + came[:, width:]
        )
    return state


def by_blocks(source, attention_group_count, position_count):
    return (
        source.astype(jnp.float32)
        .reshape(attention_group_count, HEAD, position_count // BLOCK, BLOCK)
        .transpose(0, 2, 3, 1)
    )


def compose(earlier, latter):
    return (
        jnp.einsum("...ij,...jk->...ik", earlier[0], latter[0], precision=high),
        jnp.einsum("...ij,...jk->...ik", earlier[1], latter[0], precision=high) + latter[1],
    )


def unit_lower_solve(mutual, right_side):
    power = -mutual
    solved = right_side
    for level in range((BLOCK - 1).bit_length()):
        solved = solved + jnp.einsum("hbts,hbsn->hbtn", power, solved, precision=highest)
        if level + 1 < (BLOCK - 1).bit_length():
            power = jnp.einsum("hbts,hbsu->hbtu", power, power, precision=highest)
    return solved


def rms_rows(middle, dense_block_scaler):
    scale_rows = lax.rsqrt(jnp.mean(middle * middle, axis=-1, keepdims=True) + norm_eps)
    return (middle * scale_rows * dense_block_scaler).astype(jnp.bfloat16)


def local(
    residual_matrix,
    query_vectors,
    lookup_vectors,
    payload_vectors,
    fading_dependent_term,
    step_size_preactivation,
    attention_result_switch,
    fading_bias_vector,
    surplus_forgetting,
    per_group_scaler,
    attention_result_matrix,
    dense_block_scaler,
    switching_matrix,
    expanding_matrix,
    contracting_matrix,
):
    count_sp, count_tp = lax.axis_size("sp"), lax.axis_size("tp")
    parity = lax.axis_index("sp") % 2
    ring_place = lax.axis_index("sp") // 2
    units = switching_matrix.shape[1] // 2

    def part(x, which, axis):
        return lax.dynamic_slice_in_dim(x, which * units, units, axis)

    def gate_up(which):
        return jnp.concatenate(
            [part(switching_matrix, which, 1), part(expanding_matrix, which, 1)], axis=1
        )

    wide_pieces = around(gate_up(parity), paired(gate_up(1 - parity)))
    down_pieces = around(
        part(contracting_matrix, parity, 0), part(contracting_matrix, 1 - parity, 0)
    )
    attention_group_count = surplus_forgetting.shape[0]
    position_count = surplus_forgetting.shape[1]
    block_count = position_count // BLOCK
    read_rows = by_blocks(query_vectors, attention_group_count, position_count)
    key_rows = by_blocks(lookup_vectors, attention_group_count, position_count)
    value_rows = by_blocks(payload_vectors, attention_group_count, position_count)
    fading_preactivation = by_blocks(
        fading_dependent_term, attention_group_count, position_count
    ) + fading_bias_vector.reshape(attention_group_count, 1, 1, HEAD)
    log_fading_factor = -jnp.exp(
        -jax.nn.softplus(-fading_preactivation) - 0.5
    ) + surplus_forgetting.reshape(attention_group_count, block_count, BLOCK, 1)
    learn_rate = jax.nn.sigmoid(
        by_blocks(step_size_preactivation, attention_group_count, position_count)
    )
    unit_keys = key_rows * lax.rsqrt(jnp.sum(key_rows * key_rows, axis=-1, keepdims=True) + key_eps)
    scaled = key_rows * learn_rate
    removal = unit_keys * learn_rate
    cum_after = jnp.cumsum(log_fading_factor, axis=2)
    before = cum_after - log_fading_factor
    cum_final = cum_after[:, :, -1:, :]
    probe_keys = unit_keys * jnp.exp(before)
    removal_in = removal * jnp.exp(-cum_after)
    scaled_in = scaled * jnp.exp(-cum_after)
    reads_out = read_rows * jnp.exp(cum_after)
    position = jnp.arange(BLOCK)
    strict = position[:, None] > position[None, :]
    up_to = position[:, None] >= position[None, :]
    mutual = jnp.where(
        strict, jnp.einsum("hbtn,hbsn->hbts", probe_keys, removal_in, precision=high), 0.0
    )
    through = jnp.where(
        strict, jnp.einsum("hbtn,hbsn->hbts", probe_keys, scaled_in, precision=high), 0.0
    )
    right_side = jnp.concatenate(
        [probe_keys, jnp.einsum("hbts,hbsn->hbtn", through, value_rows, precision=high)], axis=-1
    )
    solved = unit_lower_solve(mutual, right_side)
    basis_part = solved[..., :HEAD]
    offset = solved[..., HEAD:]
    removal_end = removal * jnp.exp(cum_final - cum_after)
    scaled_end = scaled * jnp.exp(cum_final - cum_after)
    carry_map = jnp.eye(HEAD, dtype=jnp.float32) * jnp.exp(cum_final) - jnp.einsum(
        "hbtk,hbtj->hbkj", basis_part, removal_end, precision=high
    )
    carry_add = jnp.einsum(
        "hbtv,hbtj->hbvj", value_rows, scaled_end, precision=high
    ) - jnp.einsum("hbtv,hbtj->hbvj", offset, removal_end, precision=high)
    summary = (carry_map[:, 0], carry_add[:, 0])
    for block in range(1, block_count):
        summary = compose(summary, (carry_map[:, block], carry_add[:, block]))
    carried = carried_in(summary)
    starts = [carried]
    for block in range(block_count - 1):
        carried = (
            jnp.einsum("hvk,hkj->hvj", carried, carry_map[:, block], precision=high)
            + carry_add[:, block]
        )
        starts.append(carried)
    starts = jnp.stack(starts, axis=1)
    removed = -jnp.einsum("hbtk,hbvk->hbtv", basis_part, starts, precision=high) - offset
    reach_removal = jnp.where(
        up_to, jnp.einsum("hbtn,hbsn->hbts", reads_out, removal_in, precision=high), 0.0
    )
    reach_value = jnp.where(
        up_to, jnp.einsum("hbtn,hbsn->hbts", reads_out, scaled_in, precision=high), 0.0
    )
    outputs = (
        jnp.einsum("hbtk,hbvk->hbtv", reads_out, starts, precision=high)
        + jnp.einsum("hbts,hbsv->hbtv", reach_removal, removed, precision=high)
        + jnp.einsum("hbts,hbsv->hbtv", reach_value, value_rows, precision=high)
    )
    centred = outputs - jnp.mean(outputs, axis=-1, keepdims=True)
    normed_heads = centred * lax.rsqrt(
        jnp.mean(centred * centred, axis=-1, keepdims=True) + group_eps
    )
    normed_heads = normed_heads.transpose(0, 3, 1, 2).reshape(
        attention_group_count * HEAD, position_count
    )
    mixed_out = (
        normed_heads * per_group_scaler[:, None] * attention_result_switch.astype(jnp.float32)
    ).astype(jnp.bfloat16)
    tp_place = lax.axis_index("tp")
    rows = residual_matrix.shape[0]
    partial = jnp.einsum(
        "ct,cd->td", mixed_out, attention_result_matrix, preferred_element_type=jnp.float32
    )

    def rows_of(x, by):
        owner = (tp_place + by) % count_tp
        return lax.dynamic_slice_in_dim(x, owner * rows, rows, 0)

    sent = partial.astype(jnp.bfloat16)
    middle = residual_matrix.astype(jnp.float32) + rows_of(partial, 0)
    for by in range(1, count_tp):
        middle = middle + shifted(rows_of(sent, by), "tp", by).astype(jnp.float32)
    normed = rms_rows(middle, dense_block_scaler)
    depth = switching_matrix.shape[0]

    def column_blocks(x):
        return [x[:, i * depth : (i + 1) * depth] for i in range(x.shape[1] // depth)]

    turned = rolled(normed, ring_place * 2 * depth)
    blocks = column_blocks(turned)
    flipped = jnp.concatenate([blocks[i ^ 1] for i in range(count_sp)], axis=1)
    near = jnp.where(parity == 0, turned, flipped)
    far = paired(jnp.where(parity == 0, flipped, turned))

    def spread(x):
        return jnp.concatenate([x] + [shifted(x, "tp", by) for by in range(1, count_tp)], axis=0)

    def stacked(pieces):
        return jnp.concatenate([x for pair in zip(*pieces) for x in pair], axis=0)

    wide_weight = stacked(wide_pieces)

    def units_of(x):
        both = jnp.dot(x, wide_weight, preferred_element_type=jnp.float32)
        return (jax.nn.silu(both[:, :units]) * both[:, units:]).astype(jnp.bfloat16)

    near_units = units_of(spread(near))
    near_sent = paired(near_units)
    far_units = units_of(spread(far))
    far_sent = paired(far_units)
    down_own = jnp.concatenate(down_pieces[0], axis=1)
    down_other = jnp.concatenate(down_pieces[1], axis=1)

    def summed(own, other):
        product = (
            jnp.dot(own, down_own, preferred_element_type=jnp.float32)
            + jnp.dot(other, down_other, preferred_element_type=jnp.float32)
        ).astype(jnp.bfloat16)
        total = product[:rows].astype(jnp.float32)
        for by in range(1, count_tp):
            total = total + shifted(product[by * rows : (by + 1) * rows], "tp", -by).astype(
                jnp.float32
            )
        return total

    far_sum = paired(summed(far_units, near_sent).astype(jnp.bfloat16)).astype(jnp.float32)
    near_sum = summed(near_units, far_sent)
    even = column_blocks(jnp.where(parity == 0, near_sum, far_sum))
    odd = column_blocks(jnp.where(parity == 0, far_sum, near_sum))
    columns = jnp.concatenate([x for pair in zip(even, odd) for x in pair], axis=1)
    channel_out = rolled(columns, (count_sp // 2 - ring_place) % (count_sp // 2) * 2 * depth)
    return (middle + channel_out).astype(jnp.bfloat16)


LANES = 128
PAIR = 2
CUTS = 4
MESH = pl.DeviceIdType.MESH
f32, bf16 = jnp.float32, jnp.bfloat16
NN = (((1,), (0,)), ((), ()))
NT = (((1,), (1,)), ((), ()))


def mm(a, b, dims=NN):
    return lax.dot_general(a, b, dims, preferred_element_type=f32)


def split(x):
    top = x.astype(bf16)
    return top, (x - top.astype(f32)).astype(bf16)


def mm3(a, b, dims=NN):
    (ah, al), (bh, bl) = split(a), split(b)
    axis = dims[0][1][0]
    return mm(
        jnp.concatenate([ah, al], axis=1), jnp.concatenate([bh, bh], axis=axis), dims
    ) + mm(ah, bl, dims)


def mm2(a, b, dims=NN):
    axis = dims[0][1][0]
    return mm(
        jnp.concatenate([a, a], axis=1), jnp.concatenate(split(b), axis=axis), dims
    )


def grid_of(rows):
    return (
        lax.broadcasted_iota(jnp.int32, (rows, LANES), 0),
        lax.broadcasted_iota(jnp.int32, (rows, LANES), 1),
    )


def heads_apart(x):
    row, col = grid_of(LANES)
    return jnp.where((row < HEAD) == (col < HEAD), jnp.concatenate([x, x], axis=0), 0.0)


def inverses(mutuals):
    row, col = grid_of(LANES)
    eye = jnp.where(row == col, 1.0, 0.0)
    solved = [eye - jnp.where((row % 2 == 0) & (col == row + 1), a, 0.0) for a in mutuals]
    for level in range(1, LANES.bit_length() - 1):
        size = 1 << level
        cross = ((row // size) % 2 == 0) & (col // size == row // size + 1)
        rounded = [s.astype(bf16) for s in solved]
        moved = [
            mm(r, jnp.where(cross, a, 0.0).astype(bf16)).astype(bf16)
            for r, a in zip(rounded, mutuals)
        ]
        solved = [s - mm(m, r) for s, m, r in zip(solved, moved, rounded)]
    rest = [eye - s - mm3(a, s) for a, s in zip(mutuals, solved)]
    return [s + mm(s.astype(bf16), r.astype(bf16)) for s, r in zip(solved, rest)]


def layer_kernel(
    zn,
    resid, query, key, value, fading, step_size, switch, bias, surplus, head_gain, row_gain,
    wo, wg, wu, wd,
    out,
    wo_v, gbuf, ubuf, dbuf,
    solved_s, reach_r, reach_v, reads_s, map_s, add_s, read_map, read_add,
    own_sum, sum_out, sum_in, pair_sum, state_out, state_in, entering,
    mixed, part, kept, core_out, core_in, y_out, y_in, z_out, z_in,
    middle, tokens, hidden,
    pair_out, pair_in, step_in,
    local_sem, pair_sem, step_r, wz_s, wz_r, wx_s, wx_r, sum_sem, state_sem,
    core_s, core_r, y_s, y_r, z_s, z_r,
    own_s, ring_s, ring_r, ty_s, ty_r, tc_s, tc_r, td_s, td_r,
):
    sp, tp = lax.axis_index("sp"), lax.axis_index("tp")
    z, x = sp // PAIR, sp % PAIR
    t_core = tp + 1 - 2 * (tp % 2)
    t_y = (tp + 2) % 4
    t_both = (t_core + 2) % 4
    rows, width = resid.shape
    positions = query.shape[1]
    blocks = positions // LANES
    pairs = query.shape[0] // LANES
    depth = wg.shape[0]
    tiles = wg.shape[1] // LANES
    base, spare = tiles // zn, tiles % zn
    bits = (zn - 1).bit_length()

    own_group = 0

    def is_own(g):
        return isinstance(g, int) and g == own_group

    def zx(g):
        return sum(((z // (1 << i) + g // (1 << i)) % 2) * (1 << i) for i in range(bits))

    def at(zz, xx, tt):
        return {"sp": zz * PAIR + xx, "tp": tt}

    def first_tile(zz):
        return zz * base + sum((zz + zn - 1 - i) // zn for i in range(spare))

    def longer(zz):
        return zz < spare

    def remote(src, dst, send, recv, to):
        return pltpu.make_async_remote_copy(
            src_ref=src, dst_ref=dst, send_sem=send, recv_sem=recv, device_id=to, device_id_type=MESH
        )

    x_peer, y_peer, core_peer = at(z, 1 - x, tp), at(z, x, t_y), at(z, x, t_core)

    barrier = pltpu.get_barrier_semaphore()
    peers = [x_peer, y_peer, core_peer] + [at(zx(g), x, tp) for g in range(1, zn)]
    for peer in peers:
        pl.semaphore_signal(barrier, inc=1, device_id=peer, device_id_type=MESH)
    pl.semaphore_wait(barrier, len(peers))

    runs = [(0, base)] + ([(base, 1)] if spare else [])

    def run_start(zz, run):
        short = (zz + zn - spare) // zn if run[0] else 0
        return pl.multiple_of((first_tile(zz) + run[0] - short) * LANES, LANES)

    def wide(ref, zz, run):
        first = run_start(zz, run)
        return ref.at[:, pl.ds(first, run[1] * LANES)]

    def tall(ref, zz, run):
        first = run_start(zz, run)
        return ref.at[pl.ds(first, run[1] * LANES), :]

    def slots(place):
        span = pl.ds(pl.multiple_of(place * depth, depth), depth)
        units = [slice(a * LANES, (a + n) * LANES) for a, n in runs]
        return (
            [w.at[span, u] for u in units for w in (gbuf, ubuf)]
            + [dbuf.at[u, span] for u in units]
        )

    def cut(zz):
        return [wide(w, zz, run) for run in runs for w in (wg, wu)] + [
            tall(wd, zz, run) for run in runs
        ]

    is_spare = [False, False, True, True, False, True] if spare else [False] * 3
    count = len(is_spare)
    every, wide_two, tall_one = range(count), range(count * 2 // 3), range(count * 2 // 3, count)

    def each(copies, which, zz, action):
        for i in which:
            if is_spare[i]:
                pl.when(longer(zz))(functools.partial(action, copies[i]))
            else:
                action(copies[i])

    def begin(copies, which, zz):
        each(copies, which, zz, lambda c: c.start())

    wo_copy = pltpu.make_async_copy(wo, wo_v, local_sem.at[count])
    own_copies = [
        pltpu.make_async_copy(a, b, local_sem.at[i])
        for i, (a, b) in enumerate(zip(cut(z), slots(sp)))
    ]

    def z_weights(g):
        return [
            remote(a, b, wz_s.at[g, i], wz_r.at[g, i], at(zx(g), x, tp))
            for i, (a, b) in enumerate(zip(cut(zx(g)), slots(sp)))
        ]

    def x_weights(g):
        there = slots(zx(g) * PAIR + x)
        return [
            remote(a, b, wx_s.at[g, i], wx_r.at[g, i], x_peer)
            for i, (a, b) in enumerate(zip(cut(z) if is_own(g) else there, there))
        ]

    def column(ref, hp):
        return jnp.broadcast_to(ref[pl.ds(hp, 1), :], (LANES, LANES)).T

    def column(ref, hp):
        return jnp.broadcast_to(ref[pl.ds(hp, 1), :], (LANES, LANES)).T

    def start_up(g, which):
        pl.when(zx(g) > z)(lambda: begin(z_weights(g), which, zx(g)))

    def start_down(g, which):
        pl.when(zx(g) < z)(lambda: begin(z_weights(g), which, zx(g)))

    def forward(g, which):
        onward = dict(zip(every, x_weights(g)))
        came = z_weights(g)

        def move(i):
            came[i].wait_recv()
            onward[i].start()

        each(list(every), which, z, move)

    inner = ((z + 1) // 2) % 2
    rest = list(range(4, zn))
    arrive = [3 - inner, 1, 2 + inner] + rest if zn >= 4 else [1]
    pieces = [1, 2 + inner, 3 - inner] + rest if zn >= 4 else [1]

    far_first = list(range(zn - 1, 0, -1))
    wo_copy.start()
    begin(own_copies, every, z)
    begin(x_weights(0), every, z)
    if zn >= 4:

        @pl.when(inner == 1)
        def _():
            for g in [2, 3, 1] + rest:
                start_down(g, every)

        @pl.when(inner == 0)
        def _():
            for g in far_first:
                start_down(g, every)

    else:
        start_down(1, every)

    @pl.when(z == 0)
    def _():
        for g in far_first[:-1]:
            begin(z_weights(g), every, zx(g))

    if spare:

        @pl.when(z >= spare)
        def _():
            gbuf[:, base * LANES :] = jnp.zeros((width, LANES), bf16)
            ubuf[:, base * LANES :] = jnp.zeros((width, LANES), bf16)
            dbuf[base * LANES :, :] = jnp.zeros((LANES, width), bf16)

    row, col = grid_of(LANES)
    strict, up_to = row < col, row <= col
    row_h, col_h = grid_of(HEAD)
    left = col_h < HEAD

    def prepared(hp, mutuals, grams):
        r0 = pl.multiple_of(hp * LANES, LANES)
        here = pl.ds(r0, LANES)
        keys = key[here, :].astype(f32)
        extra = jnp.concatenate(
            [
                jnp.broadcast_to(surplus[pl.ds(2 * hp + i, 1), :], (HEAD, positions))
                for i in range(2)
            ],
            axis=0,
        )
        pre = fading[here, :].astype(f32) + jnp.tile(column(bias, hp), (1, blocks))
        log_fade = -0.6065306597126334 / (1.0 + jnp.exp(-pre)) + extra
        rate = 1.0 / (1.0 + jnp.exp(-step_size[here, :].astype(f32)))
        unit = jnp.concatenate(
            [
                h * lax.rsqrt(jnp.sum(h * h, axis=0, keepdims=True) + key_eps)
                for h in (keys[:HEAD], keys[HEAD:])
            ],
            axis=0,
        )
        removal, scaled = unit * rate, keys * rate
        reads = query[here, :].astype(f32)
        ones = jnp.where(up_to, 1.0, 0.0).astype(bf16)
        ends, probes = [], []
        for b in range(blocks):
            lanes = slice(b * LANES, (b + 1) * LANES)
            fade = log_fade[:, lanes]
            f1 = fade.astype(bf16)
            left_over = fade - f1.astype(f32)
            f2 = left_over.astype(bf16)
            f3 = (left_over - f2.astype(f32)).astype(bf16)
            after = mm(f1, ones) + (mm(f2, ones) + mm(f3, ones))
            before = after - fade
            mid, last = after[:, HEAD - 1 : HEAD], after[:, LANES - 1 :]
            shrink = jnp.exp(mid - after)
            probe = unit[:, lanes] * jnp.exp(before - mid)
            read = reads[:, lanes] * jnp.exp(after - mid)
            removal_in, scaled_in = removal[:, lanes] * shrink, scaled[:, lanes] * shrink
            to_mid, to_end = jnp.exp(mid), jnp.exp(last - mid)
            reads_s[hp * blocks + b] = read * to_mid
            probes.append(probe * to_mid)
            ends.append((removal_in * to_end, scaled_in * to_end, jnp.exp(last)))
            both_in = [split(removal_in), split(scaled_in)]
            top, low = split(jnp.concatenate([probe, read], axis=1))
            for hh in range(2):
                own = slice(hh * HEAD, (hh + 1) * HEAD)
                turned = jnp.concatenate(
                    [
                        jnp.concatenate([h[own], l[own]], axis=0).astype(f32).T.astype(bf16)
                        for h, l in both_in
                    ],
                    axis=0,
                )
                right = jnp.concatenate(
                    [top[own], top[own], low[own], jnp.zeros_like(low[own])], axis=0
                )
                gram = mm(jnp.concatenate([turned, turned], axis=1), right)
                mutuals.append(jnp.where(strict, gram[:LANES, :LANES], 0.0))
                place = (hp * blocks + b) * 2 + hh
                reach_r[place] = jnp.where(up_to, gram[:LANES, LANES:], 0.0)
                reach_v[place] = jnp.where(up_to, gram[LANES:, LANES:], 0.0)
                grams.append(jnp.where(strict, gram[LANES:, :LANES], 0.0))
        return ends, probes

    def summed(hp, ends, probes, inverse, grams):
        values = value[pl.ds(pl.multiple_of(hp * LANES, LANES), LANES), :]
        total = None
        for b in range(blocks):
            lanes = slice(b * LANES, (b + 1) * LANES)
            removal_end, scaled_end, fade_end = ends[b]
            taken_out, added = [], []
            for hh in range(2):
                own = slice(hh * HEAD, (hh + 1) * HEAD)
                vals = values[own, lanes]
                right = jnp.concatenate([probes[b][own], mm2(vals, grams[b * 2 + hh])], axis=0)
                solved = mm3(right, inverse[b * 2 + hh])
                solved_s[(hp * blocks + b) * 2 + hh] = solved
                taken_out.append(mm3(solved, removal_end, NT))
                added.append(mm2(vals, scaled_end, NT))
            both = [
                jnp.where(left, taken_out[0][i], taken_out[1][i])
                for i in (slice(0, HEAD), slice(HEAD, LANES))
            ]
            fade_both = jnp.where(left, fade_end[:HEAD], fade_end[HEAD:])
            carry_map = jnp.where(row_h == col_h % HEAD, fade_both, 0.0) - both[0]
            carry_add = jnp.where(left, added[0], added[1]) - both[1]
            map_s[hp * blocks + b] = carry_map
            add_s[hp * blocks + b] = carry_add
            if total is None:
                total = jnp.concatenate([carry_map, carry_add], axis=0)
            else:
                total = mm3(total, heads_apart(carry_map)) + jnp.concatenate(
                    [jnp.zeros_like(carry_add), carry_add], axis=0
                )
        own_sum[hp] = total
        sum_out[hp] = total.astype(bf16)

    together = 2 if pairs % 2 == 0 else 1

    def sum_copy(i):
        share = pl.ds(i * together, together)
        return remote(sum_out.at[share], sum_in.at[share], sum_sem.at[0, i], sum_sem.at[1, i], x_peer)

    def first_part(i, _):
        mutuals, grams, ready = [], [], []
        for j in range(together):
            ready.append(prepared(i * together + j, mutuals, grams))
        inverse = inverses(mutuals)
        for j in range(together):
            span = slice(j * 2 * blocks, (j + 1) * 2 * blocks)
            summed(i * together + j, *ready[j], inverse[span], grams[span])
        sum_copy(i).start()
        return _

    lax.fori_loop(0, pairs // together, first_part, 0)


    def reading_part(hp, _):
        here = pl.ds(pl.multiple_of(hp * LANES, LANES), LANES)
        for b in range(blocks):
            lanes = slice(b * LANES, (b + 1) * LANES)
            maps, adds = [], []
            reads = reads_s[hp * blocks + b]
            values = value[here, lanes]
            for hh in range(2):
                own = slice(hh * HEAD, (hh + 1) * HEAD)
                place = (hp * blocks + b) * 2 + hh
                gone = mm3(solved_s[place], reach_r[place])
                maps.append(reads[own] - gone[:HEAD])
                adds.append(mm2(values[own], reach_v[place]) - gone[HEAD:])
            read_map[hp * blocks + b] = jnp.concatenate(maps, axis=0)
            read_add[hp * blocks + b] = jnp.concatenate(adds, axis=0)
        return _

    lax.fori_loop(0, pairs, reading_part, 0)
    for i in range(pairs // together):
        sum_copy(i).wait_recv()

    def pair_part(hp, _):
        got, own = sum_in[hp].astype(f32), own_sum[hp]
        first = jnp.where(x == 0, own, got)
        second = jnp.where(x == 0, got, own)
        pair_sum[hp] = mm3(first, heads_apart(second[:HEAD])) + jnp.concatenate(
            [jnp.zeros((HEAD, LANES), f32), second[HEAD:]], axis=0
        )
        return _

    lax.fori_loop(0, pairs, pair_part, 0)
    if zn >= 4:

        @pl.when(inner == 0)
        def _():
            forward(arrive[0], every)


    up_z, down_z = (z + 1) % zn, (z + zn - 1) % zn
    state_copy = remote(state_out, state_in, state_sem.at[0], state_sem.at[1], at(up_z, x, tp))

    @pl.when(z == 0)
    def _():
        state_in[...] = jnp.zeros_like(state_in)

    @pl.when(z > 0)
    def _():
        state_copy.wait_recv()

    def chain_part(hp, _):
        state_out[hp] = (
            mm2(state_in[hp], heads_apart(pair_sum[hp, :HEAD])) + pair_sum[hp, HEAD:]
        ).astype(bf16)
        return _

    lax.fori_loop(0, pairs, chain_part, 0)

    @pl.when(z < zn - 1)
    def _():
        state_copy.start()

    @pl.when(z == 0)
    def _():
        begin(z_weights(1), wide_two, zx(1))

    @pl.when(z > 0)
    def _():
        start_up(1, every)
        if zn >= 4:
            start_up(3, wide_two)
            start_up(2, every)
            start_up(3, tall_one)
            for g in rest:
                start_up(g, every)

    if zn >= 4:

        @pl.when(inner == 1)
        def _():
            forward(arrive[0], every)

    else:
        forward(arrive[0], every)


    def second_part(hp, _):
        r0 = pl.multiple_of(hp * LANES, LANES)
        here = pl.ds(r0, LANES)
        came = state_in[hp].astype(f32)
        gain = column(head_gain, hp)
        got = sum_in[hp].astype(f32)
        state = jnp.where(x == 0, came, mm3(came, heads_apart(got[:HEAD])) + got[HEAD:])
        for b in range(blocks):
            place = hp * blocks + b
            result = mm3(heads_apart(state), read_map[place]) + read_add[place]
            normed = []
            for h in (result[:HEAD], result[HEAD:]):
                centred = h - jnp.mean(h, axis=0, keepdims=True)
                normed.append(
                    centred * lax.rsqrt(jnp.mean(centred * centred, axis=0, keepdims=True) + group_eps)
                )
            lanes = slice(b * LANES, (b + 1) * LANES)
            done = jnp.concatenate(normed, axis=0) * gain * switch[here, lanes].astype(f32)
            mixed[lanes, here] = done.T.astype(bf16)
            if b + 1 < blocks:
                state = mm3(state, heads_apart(map_s[place])) + add_s[place]
        return _

    lax.fori_loop(0, pairs, second_part, 0)

    step = 4 * LANES
    wo_copy.wait()

    def project(i, _):
        cols = pl.ds(pl.multiple_of(i * step, step), step)
        part[0, :, cols] = mm(mixed[...], wo_v[:, cols])
        return _

    lax.fori_loop(0, width // step, project, 0)

    def rows_for(t):
        return pl.ds(pl.multiple_of(t * rows, rows), rows)

    def core_copy(i, j):
        return remote(
            core_out.at[i, j], core_in.at[i, j], core_s.at[i, j], core_r.at[i, j], core_peer
        )

    cuts = [slice(i * width // CUTS, (i + 1) * width // CUTS) for i in range(CUTS)]

    def y_copy(i, h):
        return remote(
            y_out.at[i, :, cuts[h]], y_in.at[i, :, cuts[h]], y_s.at[i, h], y_r.at[i, h], y_peer
        )

    def send_core(i, buf):
        core_out[i, 1] = part[buf, rows_for(t_both), :].astype(bf16)
        core_copy(i, 1).start()
        core_out[i, 0] = part[buf, rows_for(t_core), :].astype(bf16)
        core_copy(i, 0).start()

    def send_y(i, buf):
        if is_own(i):
            pair_copy.wait_recv()
        core_copy(i, 1).wait_recv()
        for h, cols in enumerate(cuts):
            across = part[buf, rows_for(t_y), cols] + core_in[i, 1, :, cols].astype(f32)
            if beside(i):
                pair_out[1, :, cols] = across.astype(bf16)
                continue
            if is_own(i):
                across = across + pair_in[1, :, cols].astype(f32)
            y_out[i, :, cols] = across.astype(bf16)
            y_copy(i, h).start()
        core_copy(i, 0).wait_recv()
        for cols in cuts:
            along = part[buf, rows_for(tp), cols] + core_in[i, 0, :, cols].astype(f32)
            if beside(i):
                pair_out[0, :, cols] = along.astype(bf16)
                continue
            if is_own(i):
                along = along + pair_in[0, :, cols].astype(f32)
            kept[i, :, cols] = along
        if beside(i):
            pair_copy.start()

    def beside(g):
        return isinstance(g, int) and g == 1

    pair_copy = remote(pair_out, pair_in, pair_sem.at[2], pair_sem.at[3], at(zx(1), x, tp))
    send_core(zn, 0)
    send_y(zn, 0)
    for h in range(CUTS):
        y_copy(zn, h).wait_recv()
    middle[...] = resid[...].astype(f32) + (kept[zn] + y_in[zn].astype(f32))
    mid_rows = middle[...]
    scale = lax.rsqrt(jnp.mean(mid_rows * mid_rows, axis=-1, keepdims=True) + norm_eps)
    tokens[z, rows_for(tp), :] = (mid_rows * scale * row_gain[...]).astype(bf16)

    def piece(zz, t):
        return tokens.at[zz, rows_for(t), :]

    def up_copy(zz, sem):
        return remote(piece(zz, tp), piece(zz, tp), sem, ring_r.at[zz], at(up_z, x, tp))

    def down_copy(zz, sem):
        return remote(piece(zz, tp), piece(zz, tp), sem, ring_r.at[zz], at(down_z, x, tp))

    def when(cond, action):
        pl.when(cond)(action)

    def y_token(g):
        return remote(piece(zx(g), tp), piece(zx(g), tp), ty_s.at[g], ty_r.at[g], y_peer)

    def y_token_came(g):
        return remote(piece(zx(g), t_y), piece(zx(g), t_y), ty_s.at[g], ty_r.at[g], y_peer)

    def core_token(g):
        return remote(piece(zx(g), tp), piece(zx(g), tp), tc_s.at[g], tc_r.at[g], core_peer)

    def core_token_came(g):
        return remote(piece(zx(g), t_core), piece(zx(g), t_core), tc_s.at[g], tc_r.at[g], core_peer)

    def both_token(g):
        return remote(piece(zx(g), t_y), piece(zx(g), t_y), td_s.at[g], td_r.at[g], core_peer)

    def both_token_came(g):
        return remote(piece(zx(g), t_both), piece(zx(g), t_both), td_s.at[g], td_r.at[g], core_peer)

    def pair_token(zz):
        return remote(piece(zz, t_y), piece(zz, t_y), pair_sem.at[0], pair_sem.at[1], at(zx(1), x, tp))

    def spread_z(g):
        zz = zx(g)
        if is_own(g):
            when(z < zn - 1, lambda: up_copy(zz, own_s.at[0]).start())
            when(z > 0, lambda: down_copy(zz, own_s.at[1]).start())
        else:
            up_copy(zz, ring_s.at[g]).wait_recv()
            when((zz < z) & (z < zn - 1), lambda: up_copy(zz, ring_s.at[g]).start())
            when((zz > z) & (z > 0), lambda: down_copy(zz, ring_s.at[g]).start())
        if not beside(g):
            y_token(g).start()
        core_token(g).start()

    def spread_y(g):
        if beside(g):
            pair_token(zx(1)).wait_recv()
        else:
            y_token_came(g).wait_recv()
        both_token(g).start()
        if is_own(g):
            pair_token(z).start()

    spread_z(own_group)
    pl.when(z == 0)(lambda: begin(z_weights(1), tall_one, zx(1)))
    if zn > 2:
        forward(arrive[1], every)
    spread_y(0)
    for g in arrive[2:]:
        forward(g, every)
    near, far = pieces[0], pieces[1:]
    spread_z(near)
    if far:
        spread_z(far[0])

    @pl.when(inner == 1)
    def _():
        for g in far[1:]:
            spread_z(g)
        for g in pieces:
            spread_y(g)

    @pl.when(inner == 0)
    def _():
        spread_y(near)

    each(own_copies, every, z, lambda c: c.wait())
    for g in range(zn):
        each(x_weights(g), every, z, lambda c: c.wait_recv())

    def feed(g, buf):
        core_token_came(g).wait_recv()
        both_token_came(g).wait_recv()
        block = tokens[zx(g)]
        gate = mm(block, gbuf[...])
        up = mm(block, ubuf[...])
        hidden[...] = (gate / (1.0 + jnp.exp(-gate)) * up).astype(bf16)

        def down(i, _):
            cols = pl.ds(pl.multiple_of(i * step, step), step)
            part[buf, :, cols] = mm(hidden[...], dbuf[:, cols])
            return _

        lax.fori_loop(0, width // step, down, 0)

    def z_copy(g, h):
        return remote(
            z_out.at[g, :, cuts[h]], z_in.at[g, :, cuts[h]], z_s.at[g, h], z_r.at[g, h],
            at(zx(g), x, tp),
        )

    def step_copy(k, g, h):
        return remote(
            z_out.at[g, :, cuts[h]], step_in.at[k, :, cuts[h]], z_s.at[g, h], step_r.at[k, h],
            at(zx(1), x, tp),
        )

    def send_z(k, g):
        for h, cols in enumerate(cuts):
            y_copy(g, h).wait_recv()
            mine = kept[g, :, cols] + y_in[g, :, cols].astype(f32)
            if is_own(g):
                kept[g, :, cols] = mine
                continue

            @pl.when(inner == 0)
            def _():
                z_out[g, :, cols] = mine.astype(bf16)
                step_copy(k, g, h).start()

            @pl.when(inner == 1)
            def _():
                step_copy(k, g, h).wait_recv()
                z_out[g, :, cols] = (mine + step_in[k, :, cols].astype(f32)).astype(bf16)
                z_copy(g, h).start()

    feed(near, 2)
    send_core(near, 2)

    @pl.when(inner == 0)
    def _():
        for g in far[1:]:
            spread_z(g)
        send_y(near, 2)
        for g in far[:1]:
            spread_y(g)

    buf = 0
    for i, g in enumerate(far):
        buf = 1 - buf
        feed(g, buf)
        send_core(g, buf)
        if i == 0:
            pl.when(inner == 1)(lambda: send_y(near, 2))
        if i + 1 < len(far):
            send_y(g, buf)

            @pl.when(inner == 0)
            def _():
                spread_y(far[i + 1])

    if not far:
        pl.when(inner == 1)(lambda: send_y(near, 2))
    feed(own_group, 2)
    for g in far[-1:]:
        send_y(g, buf)
    send_core(own_group, 2)
    pl.when(inner == 1)(lambda: send_y(own_group, 2))
    for k, g in enumerate(far):
        if k + 1 == len(far):
            pl.when(inner == 0)(lambda: send_y(own_group, 2))
        send_z(k, g)
    send_z(0, own_group)
    for h, cols in enumerate(cuts):
        z_copy(far[0], h).wait_recv()
        total = middle[:, cols] + kept[0, :, cols] + z_in[far[0], :, cols].astype(f32)
        out[:, cols] = total.astype(bf16)

    for g in range(1, zn):
        each(z_weights(g), every, zx(g), lambda c: c.wait_send())
        for h in range(CUTS):
            if not beside(g):
                z_copy(g, h).wait_send()
        zz = zx(g)
        moved_on = ((zz < z) & (z < zn - 1)) | ((zz > z) & (z > 0))
        when(moved_on, up_copy(zz, ring_s.at[g]).wait_send)
    for g in range(zn):
        each(x_weights(g), every, z, lambda c: c.wait_send())
        if not beside(g):
            y_token(g).wait_send()
        core_token(g).wait_send()
        both_token(g).wait_send()
    for i in range(zn + 1):
        for j in range(2):
            core_copy(i, j).wait_send()
        for h in range(CUTS):
            if not beside(i):
                y_copy(i, h).wait_send()
    for i in range(pairs // together):
        sum_copy(i).wait_send()
    pair_token(z).wait_send()
    pair_copy.wait_send()
    when(z < zn - 1, state_copy.wait_send)
    when(z < zn - 1, up_copy(z, own_s.at[0]).wait_send)
    when(z > 0, down_copy(z, own_s.at[1]).wait_send)


def fits(mesh, *arrays):
    sp, tp = mesh.shape["sp"], mesh.shape["tp"]
    heads, positions = arrays[8].shape
    units = arrays[12].shape[1]
    zn = sp // PAIR
    return (
        tp == 4
        and sp % PAIR == 0
        and zn == 4
        and heads % 2 == 0
        and positions % LANES == 0
        and positions == tp * arrays[0].shape[0]
        and units % LANES == 0
        and units // LANES >= zn
        and arrays[12].shape[0] % LANES == 0
        and arrays[0].shape[1] % (4 * LANES) == 0
    )


def fused(
    residual, query, key, value, fading, step_size, switch, bias, surplus, head_gain, out_proj,
    row_gain, gate_up, expand, contract,
):
    zn = lax.axis_size("sp") // PAIR
    rows, width = residual.shape
    channels, positions = query.shape
    pairs, blocks = channels // LANES, positions // LANES
    many = pairs * blocks
    taken = -(-(gate_up.shape[1] // LANES) // zn) * LANES
    square = (LANES, LANES)
    half = (HEAD, LANES)
    vmem, dma = pltpu.VMEM, pltpu.SemaphoreType.DMA
    scratch = [
        vmem(out_proj.shape, bf16),
        vmem((width, taken), bf16),
        vmem((width, taken), bf16),
        vmem((taken, width), bf16),
        vmem((2 * many, *square), f32),
        vmem((2 * many, *square), f32),
        vmem((2 * many, *square), f32),
        vmem((many, *square), f32),
        vmem((many, *half), f32),
        vmem((many, *half), f32),
        vmem((many, *square), f32),
        vmem((many, *square), f32),
        vmem((pairs, *square), f32),
        vmem((pairs, *square), bf16),
        vmem((pairs, *square), bf16),
        vmem((pairs, *square), f32),
        vmem((pairs, *half), bf16),
        vmem((pairs, *half), bf16),
        vmem((pairs, *half), f32),
        vmem((positions, channels), bf16),
        vmem((3, positions, width), f32),
        vmem((zn + 1, rows, width), f32),
        vmem((zn + 1, 2, rows, width), bf16),
        vmem((zn + 1, 2, rows, width), bf16),
        vmem((zn + 1, rows, width), bf16),
        vmem((zn + 1, rows, width), bf16),
        vmem((zn, rows, width), bf16),
        vmem((zn, rows, width), bf16),
        vmem((rows, width), f32),
        vmem((zn, positions, width), bf16),
        vmem((positions, taken), bf16),
        vmem((2, rows, width), bf16),
        vmem((2, rows, width), bf16),
        vmem((2, rows, width), bf16),
        dma((7,)), dma((4,)), dma((2, CUTS)),
        dma((zn, 6)), dma((zn, 6)), dma((zn, 6)), dma((zn, 6)),
        dma((2, pairs)), dma((2,)),
        dma((zn + 1, 2)), dma((zn + 1, 2)), dma((zn + 1, CUTS)), dma((zn + 1, CUTS)), dma((zn, CUTS)), dma((zn, CUTS)),
        dma((2,)), dma((zn,)), dma((zn,)),
        dma((zn,)), dma((zn,)), dma((zn,)), dma((zn,)), dma((zn,)), dma((zn,)),
    ]
    inside = pl.BlockSpec(memory_space=pltpu.VMEM)
    outside = pl.BlockSpec(memory_space=pl.ANY)
    return pl.pallas_call(
        functools.partial(layer_kernel, zn),
        out_shape=jax.ShapeDtypeStruct((rows, width), bf16),
        in_specs=[inside] * 11 + [outside] * 4,
        out_specs=inside,
        scratch_shapes=scratch,
        compiler_params=pltpu.CompilerParams(
            collective_id=0, has_side_effects=True, vmem_limit_bytes=60 << 20
        ),
        name="layer",
    )(
        residual, query, key, value, fading, step_size, switch, bias.reshape(pairs, LANES), surplus,
        head_gain.reshape(pairs, LANES), row_gain[None, :], out_proj, gate_up, expand, contract,
    )


def solution(mesh):
    placed = (
        P(("sp", "tp"), None),
        P("tp", "sp"),
        P("tp", "sp"),
        P("tp", "sp"),
        P("tp", "sp"),
        P("tp", "sp"),
        P("tp", "sp"),
        P("tp"),
        P("tp", "sp"),
        P("tp"),
        P("tp", None),
        P(),
        P("sp", "tp"),
        P("sp", "tp"),
        P("tp", "sp"),
    )

    def layer(*arrays):
        return (fused if fits(mesh, *arrays) else local)(*arrays)


    return jax.shard_map(
        layer, mesh=mesh, in_specs=placed, out_specs=P(("sp", "tp"), None), check_vma=False
    )
```
